128 devices in a mesh: sp: 64 (over z, y, x), tp: 2 (over core).
Axes of the slice: x: 4, y: 4, z: 4, core: 2. Of those that a mesh axis runs over, the one named last changes fastest.
Arguments:
- stream_mid: bfloat16 [12288, 2048], P('sp'), may hold values from -6 to 6
- d_out: bfloat16 [12288, 2048], P('sp'), may hold values from -16 to 16
- route_ids: int32 [12288, 2], P('sp'), may hold values from 0 to 63, all different within a row; in each aligned block of 192 rows (0 to 191, 192 to 383, ...) at most 12 rows name the same one
- route_weights: float32 [12288, 2], P('sp'), may hold values from 0.3 to 1.5
- gate_pre: bfloat16 [12288, 2048], P('sp', 'tp'), may hold values from -6 to 6
- lru_out: bfloat16 [12288, 2048], P('sp', 'tp'), may hold values from -6 to 6
- log_decay: float32 [12288, 2048], P('sp', 'tp'), may hold values from -2.5 to 0
- w_out: bfloat16 [2048, 2048], P('tp'), may hold values from -0.125 to 0.125
- exp_gate: bfloat16 [64, 2048, 1024], P('sp', None, 'tp'), may hold values from -0.125 to 0.125
- exp_up: bfloat16 [64, 2048, 1024], P('sp', None, 'tp'), may hold values from -0.125 to 0.125
- exp_down: bfloat16 [64, 1024, 2048], P('sp', 'tp'), may hold values from -0.1875 to 0.1875
Outputs:
- grad_exp_gate: float32 [64, 2048, 1024], P('sp', None, 'tp')
- grad_exp_up: float32 [64, 2048, 1024], P('sp', None, 'tp')
- grad_exp_down: float32 [64, 1024, 2048], P('sp', 'tp')
- grad_out_proj: float32 [2048, 2048], P('sp', 'tp')
- d_gate: bfloat16 [12288, 2048], P('sp', 'tp')
- d_drive: float32 [12288, 2048], P('sp', 'tp')
- d_log_decay: float32 [12288, 2048], P('sp', 'tp')
The draws below stay inside these ranges and needn't reach their ends.
Inputs may be any that keep to these rules, and one draw needn't show every extreme that they name: `route_ids`: each row names 2 different experts; among the rows of one index of sp no expert is named by more than 12 rows, and in every draw some expert is named by exactly 12 of them.
All inputs are finite; a program needn't handle non-finite values.
Results may differ from the reference program's by a relative error of at most 0.0069.
Values may be sent and summed in bfloat16 or wider, within the bound.
No kernel may reach another device: no remote copies, remote signals or barrier semaphores. Data moves between devices by JAX's collectives and lax.ppermute only.
A program may use at most 128 MiB of HBM per device.

```python
import math
import jax
import jax.numpy as jnp
import numpy as np
from jax import lax

D = 2048
RECURRENT_WIDTH = 2048
FF_E = 1024
TOPK = 2
TOK_DEV = 192
EXPERTS = 64
SEQUENCE_TOKENS = 12288
CAP = 12
N_SP = 64
N_TP = 2


def draw_log_decay(key, part):
    key_sequence = jax.random.split(jax.random.fold_in(key, 71), 7)
    slow_rate = jax.random.uniform(key_sequence[0], (RECURRENT_WIDTH,), jnp.float32, 0.2, 0.6) / SEQUENCE_TOKENS
    fast_rate = jnp.exp(jax.random.uniform(key_sequence[1], (RECURRENT_WIDTH,), jnp.float32, jnp.log(1.0 / 100.0), jnp.log(1.0 / 30.0)))
    slow_mask = jax.random.uniform(key_sequence[2], (RECURRENT_WIDTH,), jnp.float32) < 0.5
    base_rate = jnp.where(slow_mask, slow_rate, fast_rate)
    block_count = SEQUENCE_TOKENS // TOK_DEV
    block_factor = jnp.exp(jax.random.uniform(key_sequence[3], (block_count, 1), jnp.float32, 0.0, jnp.log(2.5)))
    jitter = jnp.exp(jax.random.uniform(key_sequence[4], (SEQUENCE_TOKENS, RECURRENT_WIDTH), jnp.float32, jnp.log(0.5), jnp.log(2.0)))
    decay_speeds = base_rate[None, :] * jnp.repeat(block_factor, TOK_DEV, axis=0) * jitter
    surge_token_rows = jax.random.randint(key_sequence[5], (3,), 0, SEQUENCE_TOKENS)
    surge_token_loss = jax.random.uniform(key_sequence[6], (3, RECURRENT_WIDTH), jnp.float32, 0.2, 0.5)
    surge_token_hit = (jnp.arange(SEQUENCE_TOKENS)[:, None] == surge_token_rows[None, :]).astype(jnp.float32)
    decay_speeds = decay_speeds + jnp.dot(surge_token_hit, -jnp.log(1.0 - surge_token_loss), precision=lax.Precision.HIGHEST)
    return -decay_speeds


def strengthened(result, own_key, source, target, blocks, factor):
    def block_of(axis_at):
        return (jnp.arange(result.shape[axis_at]) // (result.shape[axis_at] // blocks)).reshape((-1,) + (1,) * (result.ndim - 1 - axis_at))

    near = jax.random.permutation(own_key, blocks)[block_of(target)]
    second = (block_of(target) + blocks // 2) % blocks
    return jnp.where((block_of(source) == near) | (block_of(source) == second), factor * result, result)


def steps_of(stream_key, shape, cuts, smallest, top_value):
    factor_of = 1.0
    for axis_at, blocks in cuts:
        steps = jax.random.uniform(jax.random.fold_in(jax.random.fold_in(stream_key, 6), axis_at), (blocks,), jnp.float32, smallest / len(cuts), top_value / len(cuts))
        factor_of = factor_of * jnp.repeat(jnp.exp(steps), shape[axis_at] // blocks).reshape((-1,) + (1,) * (len(shape) - 1 - axis_at))
    return factor_of


def shared_out(rng, own, number, rows, amount, top, limit, slope):
    order = jax.random.permutation(rng, amount)
    packed, usual = load_shares(amount, rows * top, limit, slope, True), load_shares(amount, rows * top, limit, slope, False)
    places = jnp.arange(amount)

    def named(sizes, turn):
        used = int((sizes > 0).sum())
        fixed = max(1, used // 4)
        moved = fixed + (places - fixed + turn * (used - fixed)) % max(1, amount - fixed)
        return jnp.zeros((amount,), jnp.int32).at[order[jnp.where(places < fixed, places, moved)]].set(jnp.asarray(sizes, jnp.int32))

    sizes = jnp.where(number % 4 == 0, named(packed, number // 4), named(usual, number - number // 4 - 1))
    mixed = jax.random.permutation(jax.random.fold_in(own, 3), amount)
    giver, taker = mixed[0:amount // 2 * 2:2], mixed[1:amount // 2 * 2:2]
    room = jnp.minimum(sizes[giver] - 1, limit - sizes[taker]) // 2
    room = jnp.where((giver == order[0]) | (taker == order[0]) | (sizes[taker] == 0), 0, jnp.maximum(room, 0))
    moved = jax.random.randint(jax.random.fold_in(own, 4), (amount // 2,), 0, 1 << 20) % (room + 1)
    sizes = sizes.at[giver].add(-moved).at[taker].add(moved)
    items = jnp.searchsorted(jnp.cumsum(sizes), jnp.arange(rows * top), side="right").astype(jnp.int32)
    grid = items.reshape(top, rows).T
    grid = grid[jax.random.permutation(jax.random.fold_in(own, 1), rows)]
    turn = jax.random.randint(jax.random.fold_in(own, 2), (rows, 1), 0, top)
    return jnp.take_along_axis(grid, (jnp.arange(top)[None, :] + turn) % top, axis=1)


def load_shares(amount, total, bound, slope, full):
    loads = [(1 << 20) // math.isqrt(grade ** slope) + 1 for grade in range(1, amount + 1)]
    largest = bound if full else min(bound, max(-(-total // amount), total * loads[0] // sum(loads)))
    least = 1 if total - largest >= amount - 1 else 0
    given, spare = [largest] + [least] * (amount - 1), total - largest - least * (amount - 1)
    while spare > 0:
        movable = [i for i in range(1, amount) if given[i] < largest] or [i for i in range(1, amount) if given[i] < bound]
        whole, remaining = sum([loads[i] for i in movable]), spare
        for i in movable:
            more = min(bound - given[i], max(1, remaining * loads[i] // whole), spare)
            given[i] = given[i] + more
            spare = spare - more
    return np.array(given)


def noise(rng, shape, deviation, bound, shards=(), kind=jnp.bfloat16):
    drawn = deviation * jax.random.normal(rng, shape, jnp.float32)
    if shards:
        drawn = drawn * steps_of(rng, shape, shards, -0.22, 0.18)
    return jnp.clip(drawn, -bound, bound).astype(kind)


def noise_with(stream_key, extent, spread, most, cuts, heavy, kind=jnp.bfloat16):
    entries = spread * jax.random.normal(stream_key, extent, jnp.float32)
    if cuts:
        entries = entries * steps_of(stream_key, extent, cuts, -0.22, 0.18)
    return jnp.clip(strengthened(entries, jax.random.fold_in(stream_key, 3), *heavy), -most, most).astype(kind)


def setup_inputs(seed: int = 0) -> dict:
    seeds = jax.random.split(jax.random.key(seed), 12)
    stream_mid = noise(seeds[0], (SEQUENCE_TOKENS, D), 1.0, 6.0, ((0, 64),))
    d_out = noise_with(seeds[1], (SEQUENCE_TOKENS, D), 1.0, 16.0, ((0, 64),), (0, 1, 64, 4.0))
    route_ids_keys = jax.random.split(jax.random.fold_in(seeds[2], 1), SEQUENCE_TOKENS // TOK_DEV)
    route_ids_turns = jax.random.permutation(jax.random.fold_in(seeds[2], 3), SEQUENCE_TOKENS // TOK_DEV)
    route_ids = jax.vmap(lambda own, number: shared_out(jax.random.fold_in(seeds[2], 2), own, number, TOK_DEV, EXPERTS, TOPK, CAP, 1))(route_ids_keys, route_ids_turns).reshape((SEQUENCE_TOKENS, TOPK))
    route_weights = jnp.clip(0.3 + 1.2 * jax.random.uniform(seeds[3], (SEQUENCE_TOKENS, TOPK), jnp.float32) ** steps_of(seeds[3], (SEQUENCE_TOKENS, TOPK), ((0, 64),), -0.2, 0.2), 0.3, 1.5)
    gate_pre = noise(seeds[4], (SEQUENCE_TOKENS, RECURRENT_WIDTH), 1.0, 6.0, ((0, 64), (1, 2)))
    lru_out = noise(seeds[5], (SEQUENCE_TOKENS, RECURRENT_WIDTH), 1.0, 6.0, ((0, 64), (1, 2)))
    log_decay = draw_log_decay(jax.random.fold_in(seeds[11], 71), 0)
    w_out = noise(seeds[7], (RECURRENT_WIDTH, D), RECURRENT_WIDTH ** -0.5, 0.125, ((0, 2),))
    exp_gate = noise(seeds[8], (EXPERTS, D, FF_E), D ** -0.5, 0.125, ((0, 64), (2, 2)))
    exp_up = noise(seeds[9], (EXPERTS, D, FF_E), D ** -0.5, 0.125, ((0, 64), (2, 2)))
    exp_down = noise(seeds[10], (EXPERTS, FF_E, D), FF_E ** -0.5, 0.1875, ((0, 64), (1, 2)))
    return {"stream_mid": stream_mid, "d_out": d_out, "route_ids": route_ids, "route_weights": route_weights, "gate_pre": gate_pre, "lru_out": lru_out, "log_decay": log_decay, "w_out": w_out, "exp_gate": exp_gate, "exp_up": exp_up, "exp_down": exp_down}


def reverse_recurrence(decay_rate, drive):
    coeffs = jnp.concatenate([decay_rate[1:], jnp.zeros_like(decay_rate[:1])], axis=0)

    def combine(earlier, later):
        return (earlier[0] * later[0], later[0] * earlier[1] + later[1])
    _, carried = lax.associative_scan(combine, (jnp.flip(coeffs, 0), jnp.flip(drive, 0)), axis=0)
    return jnp.flip(carried, 0)

def contract_rows(left, right):
    return lax.dot_general(left, right, (((0,), (0,)), ((), ())), preferred_element_type=jnp.float32)

def contract_cols(left, right):
    return lax.dot_general(left, right, (((1,), (1,)), ((), ())), preferred_element_type=jnp.float32)

def reference(stream_mid, d_out, route_ids, route_weights, gate_pre, lru_out, log_decay, w_out, exp_gate, exp_up, exp_down):
    token_total = d_out.shape[0]
    slot_total = N_SP * CAP
    half_units = FF_E // N_TP
    flat_ids = route_ids.reshape(-1)
    padded_stream = jnp.concatenate([stream_mid, jnp.zeros((1, D), jnp.bfloat16)], axis=0)
    scaled = (route_weights[:, :, None] * d_out.astype(jnp.float32)[:, None, :]).astype(jnp.bfloat16)
    padded_scaled = jnp.concatenate([scaled.reshape(-1, D), jnp.zeros((1, D), jnp.bfloat16)], axis=0)

    def one_expert(expert):
        found = jnp.nonzero(flat_ids == expert, size=slot_total, fill_value=token_total * TOPK)[0].astype(jnp.int32)
        inputs = padded_stream[found // TOPK]
        cotangent = padded_scaled[found]
        gate_weight = exp_gate[expert]
        up_weight = exp_up[expert]
        down_weight = exp_down[expert]
        gate_proj = jnp.dot(inputs, gate_weight, preferred_element_type=jnp.float32)
        up_proj = jnp.dot(inputs, up_weight, preferred_element_type=jnp.float32)
        gate_sigmoid = jax.nn.sigmoid(gate_proj)
        gate_act = gate_proj * gate_sigmoid
        hidden = (gate_act * up_proj).astype(jnp.bfloat16)
        back_hidden = contract_cols(cotangent, down_weight)
        grad_gate_pre = (back_hidden * up_proj * gate_sigmoid * (1.0 + gate_proj * (1.0 - gate_sigmoid))).astype(jnp.bfloat16)
        grad_up_pre = (back_hidden * gate_act).astype(jnp.bfloat16)
        grad_down = contract_rows(hidden, cotangent)
        grad_gate = contract_rows(inputs, grad_gate_pre)
        grad_up = contract_rows(inputs, grad_up_pre)
        row_sum = jnp.zeros((slot_total, D), jnp.float32)
        for piece in range(N_TP):
            lower = piece * half_units
            upper = lower + half_units
            part_back = contract_cols(grad_gate_pre[:, lower:upper], gate_weight[:, lower:upper])
            part_back = part_back + contract_cols(grad_up_pre[:, lower:upper], up_weight[:, lower:upper])
            rounded = lax.optimization_barrier(part_back.astype(jnp.bfloat16))
            row_sum = row_sum + rounded.astype(jnp.float32)
        return (grad_gate, grad_up, grad_down, row_sum.astype(jnp.bfloat16), found)
    grad_exp_gate, grad_exp_up, grad_exp_down, row_back, found_all = lax.map(one_expert, jnp.arange(EXPERTS, dtype=jnp.int32))
    collected = jnp.zeros((token_total * TOPK + 1, D), jnp.float32)
    collected = collected.at[found_all.reshape(-1)].add(row_back.reshape(-1, D).astype(jnp.float32))
    routed_back = lax.optimization_barrier(jnp.sum(collected[:-1].reshape(token_total, TOPK, D), axis=1))
    d_mid = (d_out.astype(jnp.float32) + routed_back).astype(jnp.bfloat16)
    d_gated = contract_cols(d_mid, w_out)
    state_vals = lru_out.astype(jnp.float32)
    gelu_val, gelu_back = jax.vjp(jax.nn.gelu, gate_pre.astype(jnp.float32))
    gated = (gelu_val * state_vals).astype(jnp.bfloat16)
    grad_out_proj = contract_rows(d_mid, gated)
    d_gate = gelu_back(d_gated * state_vals)[0].astype(jnp.bfloat16)
    decay_rate = jnp.exp(log_decay)
    d_drive = reverse_recurrence(decay_rate, d_gated * gelu_val)
    prev_state = jnp.concatenate([jnp.zeros_like(state_vals[:1]), state_vals[:-1]], axis=0)
    d_log_decay = d_drive * decay_rate * prev_state
    return (grad_exp_gate, grad_exp_up, grad_exp_down, grad_out_proj, d_gate, d_drive, d_log_decay)
```

```python
import functools

import jax
import jax.numpy as jnp
import numpy as np
from jax import lax
from jax.experimental import pallas as pl
from jax.experimental.pallas import tpu as pltpu
from jax.sharding import Mesh, PartitionSpec as P

BF = jnp.bfloat16
F32 = jnp.float32
SP = ("z", "y", "x")
TOK = 192
D = 2048
HALF = 1024
BLK = 256
CAP = 12
CHUNK = 24
NSP = 64
SLOTS = NSP * CHUNK
ROWS = NSP * CAP
FF = 512
GROUP = 8 * CHUNK

_perm = np.zeros((GROUP, GROUP), np.float32)
for _s in range(8):
    for _h in range(2):
        for _r in range(CAP):
            _perm[_h * 96 + _s * CAP + _r, _s * CHUNK + _h * CAP + _r] = 1.0


def dot(a, b):
    return lax.dot_general(a, b, (((1,), (0,)), ((), ())), preferred_element_type=F32)


def dot_cols(a, b):
    return lax.dot_general(a, b, (((1,), (1,)), ((), ())), preferred_element_type=F32)


def dot_rows(a, b):
    return lax.dot_general(a, b, (((0,), (0,)), ((), ())), preferred_element_type=F32)


def vm(mib):
    return pltpu.CompilerParams(vmem_limit_bytes=mib * 1024 * 1024)


def lanes(index, width=BLK):
    return pl.ds(pl.multiple_of(index * width, width), width)


def slot_columns(ids_ref):
    lane = lax.broadcasted_iota(jnp.int32, (TOK, NSP), 1)
    ids0, ids1 = ids_ref[:, 0:1], ids_ref[:, 1:2]
    hot0 = jnp.where(lane == ids0, 1.0, 0.0)
    hot1 = jnp.where(lane == ids1, 1.0, 0.0)
    row = lax.broadcasted_iota(jnp.int32, (TOK, TOK), 0)
    col = lax.broadcasted_iota(jnp.int32, (TOK, TOK), 1)
    before = jnp.where(col < row, 1.0, 0.0).astype(BF)
    rank0 = dot(before, hot0.astype(BF))
    rank1 = dot(before, hot1.astype(BF)) + jnp.sum(hot0, axis=0, keepdims=True)
    first0 = jnp.sum(hot0 * rank0, axis=1, keepdims=True)
    first1 = jnp.sum(hot1 * rank1, axis=1, keepdims=True)
    return ids0.astype(F32) * CHUNK + first0, ids1.astype(F32) * CHUNK + first1


def as_row(column):
    row = lax.broadcasted_iota(jnp.int32, (TOK, TOK), 0)
    col = lax.broadcasted_iota(jnp.int32, (TOK, TOK), 1)
    return jnp.sum(jnp.where(row == col, column, 0.0), axis=0, keepdims=True)


def pack_kernel(meta, ids_ref, w_ref, x_ref, d_ref, out_ref, sx, s0, s1):
    @pl.when(pl.program_id(0) == 0)
    def _():
        c0, c1 = slot_columns(ids_ref)
        r0, r1 = as_row(c0).astype(jnp.int32), as_row(c1).astype(jnp.int32)
        slot = lax.broadcasted_iota(jnp.int32, (SLOTS, TOK), 0)
        sx[...] = jnp.where((slot == r0) | (slot == r1), 1.0, 0.0).astype(BF)
        s0[...] = jnp.where(slot == r0 + CAP, 1.0, 0.0).astype(BF)
        s1[...] = jnp.where(slot == r1 + CAP, 1.0, 0.0).astype(BF)

    d = d_ref[...].astype(F32)
    scaled0 = (w_ref[:, 0:1] * d).astype(BF)
    scaled1 = (w_ref[:, 1:2] * d).astype(BF)
    out = dot(sx[...], x_ref[...]) + dot(s0[...], scaled0) + dot(s1[...], scaled1)
    out_ref[...] = out.astype(BF)


def pack(meta, ids, weights, stream, d_out):
    return pl.pallas_call(
        pack_kernel,
        name="pack",
        grid_spec=pltpu.PrefetchScalarGridSpec(
            num_scalar_prefetch=1,
            grid=(4,),
            in_specs=[
                pl.BlockSpec((TOK, 2), lambda j, m: (0, 0)),
                pl.BlockSpec((TOK, 2), lambda j, m: (0, 0)),
                pl.BlockSpec((TOK, BLK), lambda j, m: (0, 2 * j + m[0])),
                pl.BlockSpec((TOK, BLK), lambda j, m: (0, 2 * j + m[0])),
            ],
            out_specs=pl.BlockSpec((SLOTS, BLK), lambda j, m: (0, j)),
            scratch_shapes=[pltpu.VMEM((SLOTS, TOK), BF)] * 3,
        ),
        out_shape=jax.ShapeDtypeStruct((SLOTS, HALF), BF),
        compiler_params=vm(24),
    )(meta, ids, weights, stream, d_out)


def expert_kernel(
    meta, perm_ref, own_ref, peer_ref, wg_ref, wu_ref, wd_ref,
    hid_ref, gg_ref, gu_ref, pown_ref, ppeer_ref, xs, cs, ys,
):
    tp = meta[0]
    perm = perm_ref[...]
    for src, par in ((own_ref, tp), (peer_ref, 1 - tp)):
        for g in range(2):
            moved = dot(perm, src[g * GROUP : (g + 1) * GROUP, :]).astype(BF)
            for j in range(4):
                part = lanes(2 * j + par)
                xs[g * 96 : (g + 1) * 96, part] = moved[:96, j * BLK : (j + 1) * BLK]
                cs[g * 96 : (g + 1) * 96, part] = moved[96:, j * BLK : (j + 1) * BLK]
    x = xs[...]
    gate = dot(x, wg_ref[...])
    up = dot(x, wu_ref[...])
    back = dot_cols(cs[...], wd_ref[...])
    sig = jax.nn.sigmoid(gate)
    act = gate * sig
    hid_ref[...] = (act * up).astype(BF)
    gg = (back * up * sig * (1.0 + gate * (1.0 - sig))).astype(BF)
    gu = (back * act).astype(BF)
    gg_ref[...] = gg
    gu_ref[...] = gu
    ys[...] = (dot_cols(gg, wg_ref[...]) + dot_cols(gu, wu_ref[...])).astype(BF)
    for dst, par in ((pown_ref, tp), (ppeer_ref, 1 - tp)):
        for g in range(2):
            r = slice(g * 96, (g + 1) * 96)
            low = jnp.concatenate([ys[r, lanes(par)], ys[r, lanes(2 + par)]], axis=1)
            high = jnp.concatenate([ys[r, lanes(4 + par)], ys[r, lanes(6 + par)]], axis=1)
            both = jnp.concatenate([low, high], axis=0)
            dst[g * GROUP : (g + 1) * GROUP, :] = dot_rows(perm, both).astype(BF)


def expert(meta, perm, own, peer, wg, wu, wd):
    step = 2 * GROUP
    rows = 16 * CAP
    return pl.pallas_call(
        expert_kernel,
        name="expert",
        grid_spec=pltpu.PrefetchScalarGridSpec(
            num_scalar_prefetch=1,
            grid=(4,),
            in_specs=[
                pl.BlockSpec((GROUP, GROUP), lambda i, m: (0, 0)),
                pl.BlockSpec((step, HALF), lambda i, m: (i, 0)),
                pl.BlockSpec((step, HALF), lambda i, m: (i, 0)),
                pl.BlockSpec((D, FF), lambda i, m: (0, 0)),
                pl.BlockSpec((D, FF), lambda i, m: (0, 0)),
                pl.BlockSpec((FF, D), lambda i, m: (0, 0)),
            ],
            out_specs=[
                pl.BlockSpec((rows, FF), lambda i, m: (i, 0)),
                pl.BlockSpec((rows, FF), lambda i, m: (i, 0)),
                pl.BlockSpec((rows, FF), lambda i, m: (i, 0)),
                pl.BlockSpec((step, HALF // 2), lambda i, m: (i, 0)),
                pl.BlockSpec((step, HALF // 2), lambda i, m: (i, 0)),
            ],
            scratch_shapes=[pltpu.VMEM((rows, D), BF)] * 3,
        ),
        out_shape=[jax.ShapeDtypeStruct((ROWS, FF), BF)] * 3
        + [jax.ShapeDtypeStruct((SLOTS, HALF // 2), BF)] * 2,
        compiler_params=vm(40),
    )(meta, perm, own, peer, wg, wu, wd)


def weight_kernel(
    meta, perm_ref, own_ref, peer_ref, hid_ref, gg_ref, gu_ref, og_ref, ou_ref, od_ref, xs, cs
):
    h = pl.program_id(1)
    perm = perm_ref[...]
    for g in range(8):
        rows = slice(g * GROUP, (g + 1) * GROUP)
        src = jnp.where(h == 0, own_ref[rows, :], peer_ref[rows, :])
        moved = dot(perm, src).astype(BF)
        xs[g * 96 : (g + 1) * 96, :] = moved[:96]
        cs[g * 96 : (g + 1) * 96, :] = moved[96:]
    x = xs[...]
    og_ref[...] = dot_rows(x, gg_ref[...])
    ou_ref[...] = dot_rows(x, gu_ref[...])
    od_ref[...] = dot_rows(hid_ref[...], cs[...])


def weight_grads(meta, perm, own, peer, hid, gg, gu):
    block = lambda j, h, m: 2 * j + (h + m[0]) % 2
    return pl.pallas_call(
        weight_kernel,
        name="weight_grads",
        grid_spec=pltpu.PrefetchScalarGridSpec(
            num_scalar_prefetch=1,
            grid=(4, 2),
            in_specs=[
                pl.BlockSpec((GROUP, GROUP), lambda j, h, m: (0, 0)),
                pl.BlockSpec((SLOTS, BLK), lambda j, h, m: (0, j)),
                pl.BlockSpec((SLOTS, BLK), lambda j, h, m: (0, j)),
                pl.BlockSpec((ROWS, FF), lambda j, h, m: (0, 0)),
                pl.BlockSpec((ROWS, FF), lambda j, h, m: (0, 0)),
                pl.BlockSpec((ROWS, FF), lambda j, h, m: (0, 0)),
            ],
            out_specs=[
                pl.BlockSpec((BLK, FF), lambda j, h, m: (block(j, h, m), 0)),
                pl.BlockSpec((BLK, FF), lambda j, h, m: (block(j, h, m), 0)),
                pl.BlockSpec((FF, BLK), lambda j, h, m: (0, block(j, h, m))),
            ],
            scratch_shapes=[pltpu.VMEM((ROWS, BLK), BF)] * 2,
        ),
        out_shape=[
            jax.ShapeDtypeStruct((D, FF), F32),
            jax.ShapeDtypeStruct((D, FF), F32),
            jax.ShapeDtypeStruct((FF, D), F32),
        ],
        compiler_params=vm(32),
        cost_estimate=pl.CostEstimate(
            flops=3 * 2 * ROWS * D * FF, bytes_accessed=20_000_000, transcendentals=0
        ),
    )(meta, perm, own, peer, hid, gg, gu)


def combine_kernel(meta, ids_ref, ret_ref, d_ref, dm_ref, b0, b1, b2, b3):
    tp, z = meta[0], meta[1]
    c0, c1 = slot_columns(ids_ref)
    c0, c1 = c0.astype(jnp.int32), c1.astype(jnp.int32)
    slot = lax.broadcasted_iota(jnp.int32, (TOK, SLOTS), 1)
    for side in range(2):
        pick = (slot == c0 + side * CAP) | (slot == c1 + side * CAP)
        back = dot(jnp.where(pick, 1.0, 0.0).astype(BF), ret_ref[...])
        for k in range(2):
            j = 2 * side + k
            own = d_ref[:, lanes(2 * j + tp)].astype(F32)
            dm_ref[:, j * BLK : (j + 1) * BLK] = (own + back[:, k * BLK : (k + 1) * BLK]).astype(BF)
    for k, ref in enumerate((b0, b1, b2, b3)):
        ref[...] = dm_ref[:, lanes(lax.rem(z + k, 4))]


def combine(meta, ids, ret, d_out):
    full = lambda *shape: pl.BlockSpec(shape, lambda i, m: (0, 0))
    return pl.pallas_call(
        combine_kernel,
        name="combine",
        grid_spec=pltpu.PrefetchScalarGridSpec(
            num_scalar_prefetch=1,
            grid=(1,),
            in_specs=[full(TOK, 2), full(SLOTS, HALF // 2), full(TOK, D)],
            out_specs=[full(TOK, HALF)] + [full(TOK, BLK)] * 4,
        ),
        out_shape=[jax.ShapeDtypeStruct((TOK, HALF), BF)]
        + [jax.ShapeDtypeStruct((TOK, BLK), BF)] * 4,
        compiler_params=vm(24),
    )(meta, ids, ret, d_out)


ROOT = 0.7978845608028654
CUBE = 0.044715


def gelu_parts(x):
    t = jnp.tanh(ROOT * (x + CUBE * x * x * x))
    return 0.5 * x * (1.0 + t), t


def early_kernel(gate_ref, lru_ref, decay_ref, gated_ref, block_ref):
    value, _ = gelu_parts(gate_ref[...].astype(F32))
    gated_ref[...] = (value * lru_ref[...].astype(F32)).astype(BF)
    block_ref[...] = jnp.exp(jnp.sum(decay_ref[...], axis=0, keepdims=True))


def early(gate_pre, lru_out, log_decay):
    return pl.pallas_call(
        early_kernel,
        name="early",
        out_shape=[
            jax.ShapeDtypeStruct((TOK, HALF), BF),
            jax.ShapeDtypeStruct((1, HALF), F32),
        ],
        compiler_params=vm(16),
    )(gate_pre, lru_out, log_decay)


def scan_rows(drive_ref, decay_ref, start, visit):
    carry = start
    for tile in reversed(range(TOK // 8)):
        rows = slice(tile * 8, tile * 8 + 8)
        drive, rate = drive_ref[rows, :], decay_ref[rows, :]
        here, later = [None] * 8, [None] * 8
        for r in reversed(range(8)):
            here[r] = drive[r : r + 1] + carry
            carry = rate[r : r + 1] * here[r]
            later[r] = carry
        if visit is not None:
            visit(rows, jnp.concatenate(here, axis=0), jnp.concatenate(later, axis=0))
    return carry


def drive_kernel(
    meta, own_ref, peer_ref, w_ref, gate_ref, lru_ref, decay_ref,
    dgate_ref, drive_ref, head_ref, rate_ref,
):
    tp = meta[0]
    grad = jnp.zeros((TOK, HALF), F32)
    for ref, par in ((own_ref, tp), (peer_ref, 1 - tp)):
        for j in range(4):
            grad += dot_cols(ref[:, j * BLK : (j + 1) * BLK], w_ref[:, lanes(2 * j + par)])
    x = gate_ref[...].astype(F32)
    value, t = gelu_parts(x)
    slope = 0.5 * (1.0 + t) + 0.5 * x * (1.0 - t * t) * (ROOT * (1.0 + 3.0 * CUBE * x * x))
    dgate_ref[...] = (grad * lru_ref[...].astype(F32) * slope).astype(BF)
    drive_ref[...] = grad * value
    rate_ref[...] = jnp.exp(decay_ref[...])
    head_ref[...] = scan_rows(drive_ref, rate_ref, jnp.zeros((1, HALF), F32), None)


def drive(meta, own, peer, w_out, gate_pre, lru_out, log_decay):
    full = lambda *shape: pl.BlockSpec(shape, lambda i, m: (0, 0))
    return pl.pallas_call(
        drive_kernel,
        name="drive",
        grid_spec=pltpu.PrefetchScalarGridSpec(
            num_scalar_prefetch=1,
            grid=(1,),
            in_specs=[full(TOK, HALF), full(TOK, HALF), full(HALF, D)] + [full(TOK, HALF)] * 3,
            out_specs=[full(TOK, HALF), full(TOK, HALF), full(1, HALF)],
            scratch_shapes=[pltpu.VMEM((TOK, HALF), F32)],
        ),
        out_shape=[
            jax.ShapeDtypeStruct((TOK, HALF), BF),
            jax.ShapeDtypeStruct((TOK, HALF), F32),
            jax.ShapeDtypeStruct((1, HALF), F32),
        ],
        compiler_params=vm(32),
    )(meta, own, peer, w_out, gate_pre, lru_out, log_decay)


def finish_kernel(
    meta, links_ref, drive_ref, decay_ref, lru_ref, before_ref, dd_ref, dl_ref, rate_ref, prev_ref
):
    index = meta[2]
    carry = jnp.zeros((1, HALF), F32)
    for r in reversed(range(1, NSP)):
        head = links_ref[2 * r : 2 * r + 1, :]
        block = links_ref[2 * r + 1 : 2 * r + 2, :]
        carry = jnp.where(index < r, head + block * carry, carry)
    rate_ref[...] = jnp.exp(decay_ref[...])
    state = lru_ref[...].astype(F32)
    first = lax.broadcasted_iota(jnp.int32, (TOK, HALF), 0) == 0
    prev_ref[...] = jnp.where(first, before_ref[...].astype(F32), pltpu.roll(state, 1, 0))

    def visit(rows, here, later):
        dd_ref[rows, :] = here
        dl_ref[rows, :] = later * prev_ref[rows, :]

    scan_rows(drive_ref, rate_ref, carry, visit)


def finish(meta, links, drive_value, log_decay, lru_out, before):
    full = lambda *shape: pl.BlockSpec(shape, lambda i, m: (0, 0))
    return pl.pallas_call(
        finish_kernel,
        name="finish",
        grid_spec=pltpu.PrefetchScalarGridSpec(
            num_scalar_prefetch=1,
            grid=(1,),
            in_specs=[full(2 * NSP, HALF)] + [full(TOK, HALF)] * 3 + [full(1, HALF)],
            out_specs=[full(TOK, HALF)] * 2,
            scratch_shapes=[pltpu.VMEM((TOK, HALF), F32)] * 2,
        ),
        out_shape=[jax.ShapeDtypeStruct((TOK, HALF), F32)] * 2,
        compiler_params=vm(24),
    )(meta, links, drive_value, log_decay, lru_out, before)


def outer_kernel(meta, *refs):
    own, peer, gated, out_ref = refs[0:4], refs[4:8], refs[8:12], refs[12]
    tp, z = meta[0], meta[1]
    total_own = dot_rows(own[0][...], gated[0][...])
    total_peer = dot_rows(peer[0][:, lanes(z)], gated[0][...])
    for k in range(1, 4):
        total_own += dot_rows(own[k][...], gated[k][...])
        total_peer += dot_rows(peer[k][...], gated[k][...])
    out_ref[lanes(tp), :] = total_own.astype(BF)
    out_ref[lanes(1 - tp), :] = total_peer.astype(BF)


def outer(meta, own, peer, gated):
    full = lambda a: pl.BlockSpec(a.shape, lambda i, m: (0, 0))
    args = (*own, *peer, *gated)
    return pl.pallas_call(
        outer_kernel,
        name="outer",
        grid_spec=pltpu.PrefetchScalarGridSpec(
            num_scalar_prefetch=1,
            grid=(1,),
            in_specs=[full(a) for a in args],
            out_specs=pl.BlockSpec((2 * BLK, HALF), lambda i, m: (0, 0)),
        ),
        out_shape=jax.ShapeDtypeStruct((2 * BLK, HALF), BF),
        compiler_params=vm(24),
    )(meta, *args)


def swapped(value):
    return lax.ppermute(value, "tp", [(0, 1), (1, 0)])


def turned(value, steps):
    return lax.ppermute(value, "z", [(s, (s + steps) % 4) for s in range(4)])


def on_device(
    stream_mid, d_out, route_ids, route_weights, gate_pre, lru_out, log_decay, w_out,
    exp_gate, exp_up, exp_down,
):
    index = lax.axis_index(SP)
    meta = jnp.stack([lax.axis_index("tp"), lax.axis_index("z"), index]).astype(jnp.int32)
    perm = jnp.asarray(_perm, BF)
    gated, block = early(gate_pre, lru_out, log_decay)
    before = lax.ppermute(lru_out[-1:], SP, [(s, s + 1) for s in range(NSP - 1)])
    sent = pack(meta, route_ids, route_weights, stream_mid, d_out)
    got = lax.all_to_all(sent.reshape(NSP, CHUNK, HALF), SP, 0, 0, tiled=True)
    got = got.reshape(SLOTS, HALF)
    got_peer = swapped(got)
    all_gated = (gated, *(turned(gated, k) for k in (1, 2, 3)))
    hid, gg, gu, part_own, part_peer = expert(
        meta, perm, got, got_peer, exp_gate[0], exp_up[0], exp_down[0]
    )
    other = swapped(part_peer)
    back = (part_own.astype(F32) + other.astype(F32)).astype(BF)
    ret = lax.all_to_all(back.reshape(NSP, CHUNK, HALF // 2), SP, 0, 0, tiled=True)
    grad_gate, grad_up, grad_down = weight_grads(meta, perm, got, got_peer, hid, gg, gu)
    dm, *blocks = combine(meta, route_ids, ret.reshape(SLOTS, HALF // 2), d_out)
    dm_peer = swapped(dm)
    own = (blocks[0], *(turned(blocks[k], k) for k in (1, 2, 3)))
    d_gate, drive_value, head = drive(meta, dm, dm_peer, w_out, gate_pre, lru_out, log_decay)
    pair = jnp.concatenate([head, block], axis=0).reshape(1, 16, 128)
    links = lax.all_to_all(jnp.broadcast_to(pair, (NSP, 16, 128)), SP, 0, 0, tiled=True)
    peer = (dm_peer, *(swapped(own[k]) for k in (1, 2, 3)))
    share = outer(meta, own, peer, all_gated)
    shares = lax.all_to_all(share.reshape(16, 32, HALF), ("y", "x"), 0, 0, tiled=True)
    d_drive, d_log_decay = finish(
        meta, links.reshape(2 * NSP, HALF), drive_value, log_decay, lru_out, before
    )
    grad_out_proj = jnp.sum(shares.astype(F32), axis=0)
    return (
        grad_gate[None], grad_up[None], grad_down[None], grad_out_proj, d_gate, d_drive, d_log_decay,
    )


def solution(mesh):
    fine = Mesh(mesh.devices.reshape(4, 4, 4, 2), ("z", "y", "x", "tp"))
    tokens = P(SP, None)
    both = P(SP, "tp")
    hidden = P(SP, None, "tp")
    in_specs = (
        tokens, tokens, tokens, tokens, both, both, both, P("tp", None),
        hidden, hidden, P(SP, "tp", None),
    )
    out_specs = (hidden, hidden, P(SP, "tp", None), both, both, both, both)
    return jax.shard_map(
        on_device, mesh=fine, in_specs=in_specs, out_specs=out_specs, check_vma=False
    )
```

```python
import jax
import jax.numpy as jnp
import numpy as np
from jax import lax
from jax.experimental import pallas as pl
from jax.experimental.pallas import tpu as pltpu
from jax.sharding import Mesh, PartitionSpec as P

BF = jnp.bfloat16
F32 = jnp.float32
SP = ("z", "y", "x")
TOK = 192
D = 2048
HALF = 1024
BLK = 256
CAP = 12
CHUNK = 24
NSP = 64
SLOTS = NSP * CHUNK
ROWS = NSP * CAP
FF = 512
GROUP = 8 * CHUNK

_perm = np.zeros((GROUP, GROUP), np.float32)
for _s in range(8):
    for _h in range(2):
        for _r in range(CAP):
            _perm[_h * 96 + _s * CAP + _r, _s * CHUNK + _h * CAP + _r] = 1.0


def dot(a, b):
    return lax.dot_general(a, b, (((1,), (0,)), ((), ())), preferred_element_type=F32)


def dot_cols(a, b):
    return lax.dot_general(a, b, (((1,), (1,)), ((), ())), preferred_element_type=F32)


def dot_rows(a, b):
    return lax.dot_general(a, b, (((0,), (0,)), ((), ())), preferred_element_type=F32)


def vm(mib):
    return pltpu.CompilerParams(vmem_limit_bytes=mib * 1024 * 1024)


def lanes(index, width=BLK):
    return pl.ds(pl.multiple_of(index * width, width), width)


def slot_rows(ids_ref):
    lane = lax.broadcasted_iota(jnp.int32, (NSP, TOK), 0)
    ids0, ids1 = ids_ref[0:1, :], ids_ref[1:2, :]
    hot0 = jnp.where(lane == ids0, 1.0, 0.0)
    hot1 = jnp.where(lane == ids1, 1.0, 0.0)
    row = lax.broadcasted_iota(jnp.int32, (TOK, TOK), 0)
    col = lax.broadcasted_iota(jnp.int32, (TOK, TOK), 1)
    before = jnp.where(row < col, 1.0, 0.0).astype(BF)
    rank0 = dot(hot0.astype(BF), before)
    rank1 = dot(hot1.astype(BF), before) + jnp.sum(hot0, axis=1, keepdims=True)
    first0 = jnp.sum(hot0 * rank0, axis=0, keepdims=True)
    first1 = jnp.sum(hot1 * rank1, axis=0, keepdims=True)
    return ids0.astype(F32) * CHUNK + first0, ids1.astype(F32) * CHUNK + first1


def as_column(line):
    row = lax.broadcasted_iota(jnp.int32, (TOK, TOK), 0)
    col = lax.broadcasted_iota(jnp.int32, (TOK, TOK), 1)
    return jnp.sum(jnp.where(row == col, line, 0.0), axis=1, keepdims=True)


def whole(count):
    vmem = pl.BlockSpec(memory_space=pltpu.VMEM)
    return [pl.BlockSpec(memory_space=pltpu.SMEM)] + [vmem] * count


def cost(flops, moved=0):
    return pl.CostEstimate(flops=int(flops), bytes_accessed=int(moved), transcendentals=0)


def pack_kernel(meta, ids_ref, w_ref, x_ref, d_ref, out_ref, sx, s0, s1):
    @pl.when(pl.program_id(0) == 0)
    def _():
        r0, r1 = slot_rows(ids_ref)
        r0, r1 = r0.astype(jnp.int32), r1.astype(jnp.int32)
        slot = lax.broadcasted_iota(jnp.int32, (SLOTS, TOK), 0)
        sx[...] = jnp.where((slot == r0) | (slot == r1), 1.0, 0.0).astype(BF)
        s0[...] = jnp.where(slot == r0 + CAP, 1.0, 0.0).astype(BF)
        s1[...] = jnp.where(slot == r1 + CAP, 1.0, 0.0).astype(BF)

    d = d_ref[...].astype(F32)
    scaled0 = (as_column(w_ref[0:1, :]) * d).astype(BF)
    scaled1 = (as_column(w_ref[1:2, :]) * d).astype(BF)
    out = dot(sx[...], x_ref[...]) + dot(s0[...], scaled0) + dot(s1[...], scaled1)
    out_ref[...] = out.astype(BF)


def pack(meta, ids, weights, stream, d_out):
    return pl.pallas_call(
        pack_kernel,
        name="pack",
        grid_spec=pltpu.PrefetchScalarGridSpec(
            num_scalar_prefetch=1,
            grid=(4,),
            in_specs=[
                pl.BlockSpec((2, TOK), lambda j, m: (0, 0)),
                pl.BlockSpec((2, TOK), lambda j, m: (0, 0)),
                pl.BlockSpec((TOK, BLK), lambda j, m: (0, 2 * j + m[0])),
                pl.BlockSpec((TOK, BLK), lambda j, m: (0, 2 * j + m[0])),
            ],
            out_specs=pl.BlockSpec((SLOTS, BLK), lambda j, m: (0, j)),
            scratch_shapes=[pltpu.VMEM((SLOTS, TOK), BF)] * 3,
        ),
        out_shape=jax.ShapeDtypeStruct((SLOTS, HALF), BF),
        compiler_params=vm(12),
    )(meta, ids, weights, stream, d_out)


def compact(perm, src_ref, xs, cs):
    for g in range(8):
        moved = dot(perm, src_ref[g * GROUP : (g + 1) * GROUP, :]).astype(BF)
        xs[g * 96 : (g + 1) * 96, :] = moved[:96]
        cs[g * 96 : (g + 1) * 96, :] = moved[96:]


def projections(par, xs, cs, wg_ref, wu_ref, wd_ref):
    gate = up = back = 0.0
    for j in range(4):
        mine, part = slice(j * BLK, (j + 1) * BLK), lanes(2 * j + par)
        gate += dot(xs[:, mine], wg_ref[part, :])
        up += dot(xs[:, mine], wu_ref[part, :])
        back += dot_cols(cs[:, mine], wd_ref[:, part])
    return gate, up, back


def returned(par, perm_t, gg_ref, gu_ref, wg_ref, wu_ref, ys, dst_ref):
    gg, gu = gg_ref[...], gu_ref[...]
    for j in range(4):
        part = lanes(2 * j + par)
        y = dot_cols(gg, wg_ref[part, :]) + dot_cols(gu, wu_ref[part, :])
        ys[j // 2, :, (j % 2) * BLK : (j % 2 + 1) * BLK] = y.astype(BF)
    for g in range(8):
        rows = slice(g * 96, (g + 1) * 96)
        both = jnp.concatenate([ys[0, rows, :], ys[1, rows, :]], axis=0)
        dst_ref[g * GROUP : (g + 1) * GROUP, :] = dot(perm_t, both).astype(BF)


def own_kernel(meta, perm_ref, own_ref, wg_ref, wu_ref, wd_ref, pg_ref, pu_ref, pb_ref, xs, cs):
    compact(perm_ref[...], own_ref, xs, cs)
    gate, up, back = projections(meta[0], xs, cs, wg_ref, wu_ref, wd_ref)
    pg_ref[...] = gate
    pu_ref[...] = up
    pb_ref[...] = back


def expert_own(meta, perm, own, wg, wu, wd):
    return pl.pallas_call(
        own_kernel,
        name="expert_own",
        in_specs=whole(5),
        out_specs=[pl.BlockSpec(memory_space=pltpu.VMEM)] * 3,
        out_shape=[jax.ShapeDtypeStruct((ROWS, FF), F32)] * 3,
        scratch_shapes=[pltpu.VMEM((ROWS, HALF), BF)] * 2,
        compiler_params=vm(16),
        cost_estimate=cost(4e9),
    )(meta, perm, own, wg, wu, wd)


def peer_kernel(
    meta, perm_ref, perm_t_ref, peer_ref, wg_ref, wu_ref, wd_ref, pg_ref, pu_ref, pb_ref,
    hid_ref, gg_ref, gu_ref, part_ref, xs, cs, ys,
):
    par = 1 - meta[0]
    compact(perm_ref[...], peer_ref, xs, cs)
    gate, up, back = projections(par, xs, cs, wg_ref, wu_ref, wd_ref)
    gate += pg_ref[...]
    up += pu_ref[...]
    back += pb_ref[...]
    sig = jax.nn.sigmoid(gate)
    act = gate * sig
    hid_ref[...] = (act * up).astype(BF)
    gg_ref[...] = (back * up * sig * (1.0 + gate * (1.0 - sig))).astype(BF)
    gu_ref[...] = (back * act).astype(BF)
    returned(par, perm_t_ref[...], gg_ref, gu_ref, wg_ref, wu_ref, ys, part_ref)


def expert_peer(meta, perm, perm_t, peer, wg, wu, wd, pg, pu, pb):
    return pl.pallas_call(
        peer_kernel,
        name="expert_peer",
        in_specs=whole(9),
        out_specs=[pl.BlockSpec(memory_space=pltpu.VMEM)] * 4,
        out_shape=[jax.ShapeDtypeStruct((ROWS, FF), BF)] * 3
        + [jax.ShapeDtypeStruct((SLOTS, HALF // 2), BF)],
        scratch_shapes=[pltpu.VMEM((ROWS, HALF), BF)] * 2 + [pltpu.VMEM((2, ROWS, HALF // 2), BF)],
        compiler_params=vm(20),
        cost_estimate=cost(6e9),
    )(meta, perm, perm_t, peer, wg, wu, wd, pg, pu, pb)


def back_kernel(meta, perm_t_ref, gg_ref, gu_ref, wg_ref, wu_ref, part_ref, ys):
    returned(meta[0], perm_t_ref[...], gg_ref, gu_ref, wg_ref, wu_ref, ys, part_ref)


def expert_back(meta, perm_t, gg, gu, wg, wu):
    return pl.pallas_call(
        back_kernel,
        name="expert_back",
        in_specs=whole(5),
        out_specs=pl.BlockSpec(memory_space=pltpu.VMEM),
        out_shape=jax.ShapeDtypeStruct((SLOTS, HALF // 2), BF),
        scratch_shapes=[pltpu.VMEM((2, ROWS, HALF // 2), BF)],
        compiler_params=vm(16),
        cost_estimate=cost(3e9),
    )(meta, perm_t, gg, gu, wg, wu)


def weight_kernel(
    meta, perm_ref, own_ref, peer_ref, hid_ref, gg_ref, gu_ref, og_ref, ou_ref, od_ref, xs, cs
):
    h = pl.program_id(1)
    perm = perm_ref[...]
    for g in range(8):
        rows = slice(g * GROUP, (g + 1) * GROUP)
        src = jnp.where(h == 0, own_ref[rows, :], peer_ref[rows, :])
        moved = dot(perm, src).astype(BF)
        xs[g * 96 : (g + 1) * 96, :] = moved[:96]
        cs[g * 96 : (g + 1) * 96, :] = moved[96:]
    x = xs[...]
    og_ref[...] = dot_rows(x, gg_ref[...])
    ou_ref[...] = dot_rows(x, gu_ref[...])
    od_ref[...] = dot_rows(hid_ref[...], cs[...])


def weight_grads(meta, perm, own, peer, hid, gg, gu):
    block = lambda j, h, m: 2 * j + (h + m[0]) % 2
    return pl.pallas_call(
        weight_kernel,
        name="weight_grads",
        grid_spec=pltpu.PrefetchScalarGridSpec(
            num_scalar_prefetch=1,
            grid=(4, 2),
            in_specs=[
                pl.BlockSpec((GROUP, GROUP), lambda j, h, m: (0, 0)),
                pl.BlockSpec((SLOTS, BLK), lambda j, h, m: (0, j)),
                pl.BlockSpec((SLOTS, BLK), lambda j, h, m: (0, j)),
                pl.BlockSpec((ROWS, FF), lambda j, h, m: (0, 0)),
                pl.BlockSpec((ROWS, FF), lambda j, h, m: (0, 0)),
                pl.BlockSpec((ROWS, FF), lambda j, h, m: (0, 0)),
            ],
            out_specs=[
                pl.BlockSpec((BLK, FF), lambda j, h, m: (block(j, h, m), 0)),
                pl.BlockSpec((BLK, FF), lambda j, h, m: (block(j, h, m), 0)),
                pl.BlockSpec((FF, BLK), lambda j, h, m: (0, block(j, h, m))),
            ],
            scratch_shapes=[pltpu.VMEM((ROWS, BLK), BF)] * 2,
        ),
        out_shape=[
            jax.ShapeDtypeStruct((D, FF), F32),
            jax.ShapeDtypeStruct((D, FF), F32),
            jax.ShapeDtypeStruct((FF, D), F32),
        ],
        compiler_params=vm(18),
        cost_estimate=pl.CostEstimate(
            flops=3 * 2 * ROWS * D * FF, bytes_accessed=20_000_000, transcendentals=0
        ),
    )(meta, perm, own, peer, hid, gg, gu)


def combine_kernel(meta, ids_ref, ret_ref, d_ref, dm_ref, b0, b1, b2, b3):
    tp, z = meta[0], meta[1]
    r0, r1 = slot_rows(ids_ref)
    c0, c1 = as_column(r0).astype(jnp.int32), as_column(r1).astype(jnp.int32)
    slot = lax.broadcasted_iota(jnp.int32, (TOK, SLOTS), 1)
    for side in range(2):
        pick = (slot == c0 + side * CAP) | (slot == c1 + side * CAP)
        back = dot(jnp.where(pick, 1.0, 0.0).astype(BF), ret_ref[...])
        for k in range(2):
            j = 2 * side + k
            own = d_ref[:, lanes(2 * j + tp)].astype(F32)
            dm_ref[:, j * BLK : (j + 1) * BLK] = (own + back[:, k * BLK : (k + 1) * BLK]).astype(BF)
    for k, ref in enumerate((b0, b1, b2, b3)):
        ref[...] = dm_ref[:, lanes(lax.rem(z + k, 4))]


def combine(meta, ids, ret, d_out):
    return pl.pallas_call(
        combine_kernel,
        name="combine",
        in_specs=whole(3),
        out_specs=[pl.BlockSpec(memory_space=pltpu.VMEM)] * 5,
        out_shape=[jax.ShapeDtypeStruct((TOK, HALF), BF)]
        + [jax.ShapeDtypeStruct((TOK, BLK), BF)] * 4,
        compiler_params=vm(16),
        cost_estimate=cost(1e9),
    )(meta, ids, ret, d_out)


ROOT = 0.7978845608028654
CUBE = 0.044715


def gelu_parts(x):
    t = jnp.tanh(ROOT * (x + CUBE * x * x * x))
    return 0.5 * x * (1.0 + t), t


def tile_of(line):
    return jnp.concatenate([line[:, k * 128 : (k + 1) * 128] for k in range(8)], axis=0)


def line_of(tile):
    return jnp.concatenate([tile[k : k + 1, :] for k in range(8)], axis=1)


def early_kernel(gate_ref, lru_ref, gated_ref):
    value, _ = gelu_parts(gate_ref[...].astype(F32))
    gated_ref[...] = (value * lru_ref[...].astype(F32)).astype(BF)


def early(gate_pre, lru_out):
    return pl.pallas_call(
        early_kernel,
        name="early",
        out_shape=jax.ShapeDtypeStruct((TOK, HALF), BF),
        compiler_params=vm(4),
        cost_estimate=cost(1e8),
    )(gate_pre, lru_out)


def scan_rows(drive_ref, rate_ref, start, visit):
    carry = start
    for tile in reversed(range(TOK // 8)):
        rows = slice(tile * 8, tile * 8 + 8)
        drive, rate = drive_ref[rows, :], rate_ref[rows, :]
        here, later = [None] * 8, [None] * 8
        for r in reversed(range(8)):
            here[r] = drive[r : r + 1] + carry
            carry = rate[r : r + 1] * here[r]
            later[r] = carry
        if visit is not None:
            visit(rows, jnp.concatenate(here, axis=0), jnp.concatenate(later, axis=0))
    return carry


def drive_kernel(
    meta, own_ref, peer_ref, w_ref, gate_ref, lru_ref, decay_ref,
    dgate_ref, drive_ref, head_ref, rate_ref,
):
    tp = meta[0]
    grad = 0.0
    for ref, par in ((own_ref, tp), (peer_ref, 1 - tp)):
        for j in range(4):
            grad += dot_cols(ref[:, j * BLK : (j + 1) * BLK], w_ref[:, lanes(2 * j + par)])
    x = gate_ref[...].astype(F32)
    value, t = gelu_parts(x)
    slope = 0.5 * (1.0 + t) + 0.5 * x * (1.0 - t * t) * (ROOT * (1.0 + 3.0 * CUBE * x * x))
    dgate_ref[...] = (grad * lru_ref[...].astype(F32) * slope).astype(BF)
    drive_ref[...] = grad * value
    rate_ref[...] = jnp.exp(decay_ref[...])
    head_ref[0:8, :] = tile_of(scan_rows(drive_ref, rate_ref, jnp.zeros((1, HALF), F32), None))
    head_ref[8:16, :] = tile_of(jnp.exp(jnp.sum(decay_ref[...], axis=0, keepdims=True)))


def drive(meta, own, peer, w_out, gate_pre, lru_out, log_decay):
    return pl.pallas_call(
        drive_kernel,
        name="drive",
        in_specs=whole(6),
        out_specs=[pl.BlockSpec(memory_space=pltpu.VMEM)] * 4,
        out_shape=[
            jax.ShapeDtypeStruct((TOK, HALF), BF),
            jax.ShapeDtypeStruct((TOK, HALF), F32),
            jax.ShapeDtypeStruct((16, 128), F32),
            jax.ShapeDtypeStruct((TOK, HALF), F32),
        ],
        compiler_params=vm(16),
        cost_estimate=cost(2e9),
    )(meta, own, peer, w_out, gate_pre, lru_out, log_decay)


def level_kernel(place, h0, h1, h2, h3, total_ref, rest_ref, line):
    for k, ref in enumerate((h0, h1, h2, h3)):
        line[lax.rem(place[0] + k, 4), :, :] = ref[...]
    total = within = jnp.zeros((8, 128), F32)
    product = after = jnp.ones((8, 128), F32)
    for r in reversed(range(4)):
        head, block = line[r, 0:8, :], line[r, 8:16, :]
        total = head + block * total
        product = block * product
        later = place[0] < r
        within = jnp.where(later, total, within)
        after = jnp.where(later, product, after)
    total_ref[0:8, :] = total
    total_ref[8:16, :] = product
    rest_ref[0:8, :] = within
    rest_ref[8:16, :] = after


def level(pair, axis):
    place = lax.axis_index(axis).astype(jnp.int32).reshape(1)
    others = [
        lax.ppermute(pair, axis, [(s, (s - k) % 4) for s in range(4)]) for k in (1, 2, 3)
    ]
    return pl.pallas_call(
        level_kernel,
        in_specs=whole(4),
        out_specs=[pl.BlockSpec(memory_space=pltpu.VMEM)] * 2,
        out_shape=[jax.ShapeDtypeStruct((16, 128), F32)] * 2,
        scratch_shapes=[pltpu.VMEM((4, 16, 128), F32)],
        compiler_params=vm(4),
        cost_estimate=cost(1e7),
    )(place, pair, *others)


def finish_kernel(
    rx, ry, rz, drive_ref, rate_ref, lru_ref, before_ref, dd_ref, dl_ref, prev_ref
):
    inner = ry[0:8, :] + ry[8:16, :] * rz[0:8, :]
    carry = line_of(rx[0:8, :] + rx[8:16, :] * inner)
    state = lru_ref[...].astype(F32)
    first = lax.broadcasted_iota(jnp.int32, (TOK, HALF), 0) == 0
    prev_ref[...] = jnp.where(first, before_ref[...].astype(F32), pltpu.roll(state, 1, 0))

    def visit(rows, here, later):
        dd_ref[rows, :] = here
        dl_ref[rows, :] = later * prev_ref[rows, :]

    scan_rows(drive_ref, rate_ref, carry, visit)


def finish(rests, drive_value, rate, lru_out, before):
    return pl.pallas_call(
        finish_kernel,
        name="finish",
        out_shape=[jax.ShapeDtypeStruct((TOK, HALF), F32)] * 2,
        scratch_shapes=[pltpu.VMEM((TOK, HALF), F32)],
        compiler_params=vm(8),
        cost_estimate=cost(1e9),
    )(*rests, drive_value, rate, lru_out, before)


def outer_kernel(meta, *refs):
    own, peer, gated = refs[0:4], refs[4:8], refs[8:12]
    out_ref = refs[12]
    tp, z = meta[0], meta[1]
    total_own = dot_rows(own[0][...], gated[0][...])
    total_peer = dot_rows(peer[0][:, lanes(z)], gated[0][...])
    for k in range(1, 4):
        total_own += dot_rows(own[k][...], gated[k][...])
        total_peer += dot_rows(peer[k][...], gated[k][...])
    out_ref[lanes(tp), :] = total_own.astype(BF)
    out_ref[lanes(1 - tp), :] = total_peer.astype(BF)


def outer(meta, own, peer, gated):
    return pl.pallas_call(
        outer_kernel,
        name="outer",
        in_specs=whole(12),
        out_specs=pl.BlockSpec(memory_space=pltpu.VMEM),
        out_shape=jax.ShapeDtypeStruct((2 * BLK, HALF), BF),
        compiler_params=vm(12),
        cost_estimate=cost(2e9),
    )(meta, *own, *peer, *gated)


def swapped(value):
    return lax.ppermute(value, "tp", [(0, 1), (1, 0)])


def turned(value, steps):
    return lax.ppermute(value, "z", [(s, (s + steps) % 4) for s in range(4)])


def on_device(
    stream_mid, d_out, route_ids, route_weights, gate_pre, lru_out, log_decay, w_out,
    exp_gate, exp_up, exp_down,
):
    meta = jnp.stack(
        [lax.axis_index("tp"), lax.axis_index("z"), lax.axis_index(SP), lax.axis_index(("y", "x"))]
    ).astype(jnp.int32)
    perm, perm_t = jnp.asarray(_perm, BF), jnp.asarray(_perm.T, BF)
    ids = route_ids.T
    wg, wu, wd = exp_gate[0], exp_up[0], exp_down[0]
    sent = pack(meta, ids, route_weights.T, stream_mid, d_out)
    got = lax.all_to_all(sent.reshape(NSP, CHUNK, HALF), SP, 0, 0, tiled=True)
    got = got.reshape(SLOTS, HALF)
    got_peer = swapped(got)
    gated, last = early(gate_pre, lru_out), lru_out[-1:]
    gated, last, got = lax.optimization_barrier((gated, last, got))
    turns = [turned(gated, k) for k in (1, 2, 3)]
    before = lax.ppermute(last, SP, [(s, s + 1) for s in range(NSP - 1)])
    pg, pu, pb = expert_own(meta, perm, got, wg, wu, wd)
    hid, gg, gu, part_peer = expert_peer(meta, perm, perm_t, got_peer, wg, wu, wd, pg, pu, pb)
    other = swapped(part_peer)
    part_own = expert_back(meta, perm_t, gg, gu, wg, wu)
    back = (part_own.astype(F32) + other.astype(F32)).astype(BF)
    back, before, *turns = lax.optimization_barrier((back, before, *turns))
    ret = lax.all_to_all(back.reshape(NSP, CHUNK, HALF // 2), SP, 0, 0, tiled=True)
    grad_gate, grad_up, grad_down = weight_grads(meta, perm, got, got_peer, hid, gg, gu)
    ret, grad_gate, grad_up, grad_down = lax.optimization_barrier(
        (ret, grad_gate, grad_up, grad_down)
    )
    dm, *blocks = combine(meta, ids, ret.reshape(SLOTS, HALF // 2), d_out)
    dm_peer = swapped(dm)
    own = (blocks[0], *(turned(blocks[k], k) for k in (1, 2, 3)))
    peer = (dm_peer, *(swapped(own[k]) for k in (1, 2, 3)))
    share = outer(meta, own, peer, (gated, *turns))
    shares = lax.all_to_all(share.reshape(16, 32, HALF), ("y", "x"), 0, 0, tiled=True)
    d_gate, drive_value, head, rate = drive(
        meta, dm, dm_peer, w_out, gate_pre, lru_out, log_decay
    )
    line, rest_x = level(head, "x")
    plane, rest_y = level(line, "y")
    _, rest_z = level(plane, "z")
    d_drive, d_log_decay = finish((rest_x, rest_y, rest_z), drive_value, rate, lru_out, before)
    grad_out_proj = jnp.sum(shares.astype(F32), axis=0)
    return (
        grad_gate[None], grad_up[None], grad_down[None], grad_out_proj, d_gate, d_drive, d_log_decay,
    )


def solution(mesh):
    fine = Mesh(mesh.devices.reshape(4, 4, 4, 2), ("z", "y", "x", "tp"))
    tokens = P(SP, None)
    both = P(SP, "tp")
    hidden = P(SP, None, "tp")
    in_specs = (
        tokens, tokens, tokens, tokens, both, both, both, P("tp", None),
        hidden, hidden, P(SP, "tp", None),
    )
    out_specs = (hidden, hidden, P(SP, "tp", None), both, both, both, both)
    return jax.shard_map(
        on_device, mesh=fine, in_specs=in_specs, out_specs=out_specs, check_vma=False
    )
```

```python
import jax
import jax.numpy as jnp
import numpy as np
from jax import lax
from jax.experimental import pallas as pl
from jax.experimental.pallas import tpu as pltpu
from jax.sharding import Mesh, PartitionSpec as P

BF = jnp.bfloat16
F32 = jnp.float32
SP = ("z", "y", "x")
TOK = 192
D = 2048
HALF = 1024
BLK = 256
CAP = 12
CHUNK = 24
NSP = 64
SLOTS = NSP * CHUNK
ROWS = NSP * CAP
FF = 512
GROUP = 8 * CHUNK

_perm = np.zeros((GROUP, GROUP), np.float32)
for _s in range(8):
    for _h in range(2):
        for _r in range(CAP):
            _perm[_h * 96 + _s * CAP + _r, _s * CHUNK + _h * CAP + _r] = 1.0


def dot(a, b):
    return lax.dot_general(a, b, (((1,), (0,)), ((), ())), preferred_element_type=F32)


def dot_cols(a, b):
    return lax.dot_general(a, b, (((1,), (1,)), ((), ())), preferred_element_type=F32)


def dot_rows(a, b):
    return lax.dot_general(a, b, (((0,), (0,)), ((), ())), preferred_element_type=F32)


def vm(mib):
    return pltpu.CompilerParams(vmem_limit_bytes=mib * 1024 * 1024)


def lanes(index, width=BLK):
    return pl.ds(pl.multiple_of(index * width, width), width)


def slot_rows(ids_ref):
    lane = lax.broadcasted_iota(jnp.int32, (NSP, TOK), 0)
    ids0, ids1 = ids_ref[0:1, :], ids_ref[1:2, :]
    hot0 = jnp.where(lane == ids0, 1.0, 0.0)
    hot1 = jnp.where(lane == ids1, 1.0, 0.0)
    row = lax.broadcasted_iota(jnp.int32, (TOK, TOK), 0)
    col = lax.broadcasted_iota(jnp.int32, (TOK, TOK), 1)
    before = jnp.where(row < col, 1.0, 0.0).astype(BF)
    rank0 = dot(hot0.astype(BF), before)
    rank1 = dot(hot1.astype(BF), before) + jnp.sum(hot0, axis=1, keepdims=True)
    first0 = jnp.sum(hot0 * rank0, axis=0, keepdims=True)
    first1 = jnp.sum(hot1 * rank1, axis=0, keepdims=True)
    return ids0.astype(F32) * CHUNK + first0, ids1.astype(F32) * CHUNK + first1


def as_column(line):
    row = lax.broadcasted_iota(jnp.int32, (TOK, TOK), 0)
    col = lax.broadcasted_iota(jnp.int32, (TOK, TOK), 1)
    return jnp.sum(jnp.where(row == col, line, 0.0), axis=1, keepdims=True)


def whole(count):
    vmem = pl.BlockSpec(memory_space=pltpu.VMEM)
    return [pl.BlockSpec(memory_space=pltpu.SMEM)] + [vmem] * count


def in_hbm(*values):
    return [pltpu.with_memory_space_constraint(v, pltpu.HBM) for v in values]


def mixed(*kinds):
    spaces = {"h": pltpu.HBM, "v": pltpu.VMEM}
    return [pl.BlockSpec(memory_space=pltpu.SMEM)] + [
        pl.BlockSpec(memory_space=spaces[k]) for k in "".join(kinds)
    ]


def fetch(pairs, sems):
    copies = [pltpu.make_async_copy(a, b, sems.at[k]) for k, (a, b) in enumerate(pairs)]
    for copy in copies:
        copy.start()
    return copies


def cost(flops, moved=0):
    return pl.CostEstimate(flops=int(flops), bytes_accessed=int(moved), transcendentals=0)


def pack_kernel(meta, ids_hbm, w_hbm, x_hbm, d_hbm, out_ref, ids, w, xs, ds, sems):
    tp = meta[0]
    small = [
        pltpu.make_async_copy(ids_hbm, ids, sems.at[0]),
        pltpu.make_async_copy(w_hbm, w, sems.at[1]),
    ]
    large = []
    for n, (src, dst) in enumerate(((x_hbm, xs), (d_hbm, ds))):
        for j in range(4):
            large.append(
                pltpu.make_async_copy(
                    src.at[:, lanes(2 * j + tp)],
                    dst.at[:, j * BLK : (j + 1) * BLK],
                    sems.at[2 + 4 * n + j],
                )
            )
    for copy in small + large:
        copy.start()
    for copy in small:
        copy.wait()
    r0, r1 = slot_rows(ids)
    r0, r1 = r0.astype(jnp.int32), r1.astype(jnp.int32)
    slot = lax.broadcasted_iota(jnp.int32, (SLOTS, TOK), 0)
    sx = jnp.where((slot == r0) | (slot == r1), 1.0, 0.0).astype(BF)
    s0 = jnp.where(slot == r0 + CAP, 1.0, 0.0).astype(BF)
    s1 = jnp.where(slot == r1 + CAP, 1.0, 0.0).astype(BF)
    w0, w1 = as_column(w[0:1, :]), as_column(w[1:2, :])
    for copy in large:
        copy.wait()
    for j in range(4):
        part = slice(j * BLK, (j + 1) * BLK)
        d = ds[:, part].astype(F32)
        scaled0, scaled1 = (w0 * d).astype(BF), (w1 * d).astype(BF)
        out = dot(sx, xs[:, part]) + dot(s0, scaled0) + dot(s1, scaled1)
        out_ref[:, part] = out.astype(BF)


def pack(meta, ids, weights, stream, d_out):
    hbm = pl.BlockSpec(memory_space=pltpu.HBM)
    return pl.pallas_call(
        pack_kernel,
        name="pack",
        in_specs=[pl.BlockSpec(memory_space=pltpu.SMEM)] + [hbm] * 4,
        out_specs=pl.BlockSpec(memory_space=pltpu.VMEM),
        out_shape=jax.ShapeDtypeStruct((SLOTS, HALF), BF),
        scratch_shapes=[
            pltpu.VMEM((2, TOK), jnp.int32),
            pltpu.VMEM((2, TOK), F32),
            pltpu.VMEM((TOK, HALF), BF),
            pltpu.VMEM((TOK, HALF), BF),
            pltpu.SemaphoreType.DMA((10,)),
        ],
        compiler_params=vm(12),
    )(meta, *in_hbm(ids, weights, stream, d_out))


def sum_kernel(a_ref, b_ref, out_hbm, both, sems):
    copies = []
    for k in range(4):
        rows = slice(k * 384, (k + 1) * 384)
        both[rows, :] = (a_ref[rows, :].astype(F32) + b_ref[rows, :].astype(F32)).astype(BF)
        copies.append(pltpu.make_async_copy(both.at[rows, :], out_hbm.at[rows, :], sems.at[k]))
        copies[-1].start()
    for copy in copies:
        copy.wait()


def part_sum(a, b):
    return pl.pallas_call(
        sum_kernel,
        name="part_sum",
        in_specs=[pl.BlockSpec(memory_space=pltpu.VMEM)] * 2,
        out_specs=pl.BlockSpec(memory_space=pltpu.HBM),
        out_shape=jax.ShapeDtypeStruct((SLOTS, HALF // 2), BF),
        scratch_shapes=[pltpu.VMEM((SLOTS, HALF // 2), BF), pltpu.SemaphoreType.DMA((4,))],
        compiler_params=vm(4),
    )(a, b)


def compact(perm, src_ref, xs, cs):
    for g in range(8):
        moved = dot(perm, src_ref[g * GROUP : (g + 1) * GROUP, :]).astype(BF)
        xs[g * 96 : (g + 1) * 96, :] = moved[:96]
        cs[g * 96 : (g + 1) * 96, :] = moved[96:]


def projections(par, xs, cs, wg_ref, wu_ref, wd_ref):
    gate = up = back = 0.0
    for j in range(4):
        mine, part = slice(j * BLK, (j + 1) * BLK), lanes(2 * j + par)
        gate += dot(xs[:, mine], wg_ref[part, :])
        up += dot(xs[:, mine], wu_ref[part, :])
        back += dot_cols(cs[:, mine], wd_ref[:, part])
    return gate, up, back


def returned(par, perm_t, gg_ref, gu_ref, wg_ref, wu_ref, ys, dst_ref):
    gg, gu = gg_ref[...], gu_ref[...]
    for j in range(4):
        part = lanes(2 * j + par)
        y = dot_cols(gg, wg_ref[part, :]) + dot_cols(gu, wu_ref[part, :])
        ys[j // 2, :, (j % 2) * BLK : (j % 2 + 1) * BLK] = y.astype(BF)
    for g in range(8):
        rows = slice(g * 96, (g + 1) * 96)
        both = jnp.concatenate([ys[0, rows, :], ys[1, rows, :]], axis=0)
        dst_ref[g * GROUP : (g + 1) * GROUP, :] = dot(perm_t, both).astype(BF)


def own_kernel(meta, perm_ref, own_ref, wg_ref, wu_ref, wd_ref, pg_ref, pu_ref, pb_ref, xs, cs):
    compact(perm_ref[...], own_ref, xs, cs)
    gate, up, back = projections(meta[0], xs, cs, wg_ref, wu_ref, wd_ref)
    pg_ref[...] = gate
    pu_ref[...] = up
    pb_ref[...] = back


def expert_own(meta, perm, own, wg, wu, wd):
    return pl.pallas_call(
        own_kernel,
        name="expert_own",
        in_specs=whole(5),
        out_specs=[pl.BlockSpec(memory_space=pltpu.VMEM)] * 3,
        out_shape=[jax.ShapeDtypeStruct((ROWS, FF), F32)] * 3,
        scratch_shapes=[pltpu.VMEM((ROWS, HALF), BF)] * 2,
        compiler_params=vm(16),
        cost_estimate=cost(4e9),
    )(meta, perm, own, wg, wu, wd)


def peer_kernel(
    meta, perm_ref, perm_t_ref, peer_ref, wg_ref, wu_ref, wd_ref, pg_ref, pu_ref, pb_ref,
    hid_ref, gg_ref, gu_ref, part_ref, xs, cs, ys,
):
    par = 1 - meta[0]
    compact(perm_ref[...], peer_ref, xs, cs)
    gate, up, back = projections(par, xs, cs, wg_ref, wu_ref, wd_ref)
    gate += pg_ref[...]
    up += pu_ref[...]
    back += pb_ref[...]
    sig = jax.nn.sigmoid(gate)
    act = gate * sig
    hid_ref[...] = (act * up).astype(BF)
    gg_ref[...] = (back * up * sig * (1.0 + gate * (1.0 - sig))).astype(BF)
    gu_ref[...] = (back * act).astype(BF)
    returned(par, perm_t_ref[...], gg_ref, gu_ref, wg_ref, wu_ref, ys, part_ref)


def expert_peer(meta, perm, perm_t, peer, wg, wu, wd, pg, pu, pb):
    return pl.pallas_call(
        peer_kernel,
        name="expert_peer",
        in_specs=whole(9),
        out_specs=[pl.BlockSpec(memory_space=pltpu.VMEM)] * 4,
        out_shape=[jax.ShapeDtypeStruct((ROWS, FF), BF)] * 3
        + [jax.ShapeDtypeStruct((SLOTS, HALF // 2), BF)],
        scratch_shapes=[pltpu.VMEM((ROWS, HALF), BF)] * 2 + [pltpu.VMEM((2, ROWS, HALF // 2), BF)],
        compiler_params=vm(20),
        cost_estimate=cost(6e9),
    )(meta, perm, perm_t, peer, wg, wu, wd, pg, pu, pb)


def back_kernel(meta, perm_t_ref, gg_ref, gu_ref, wg_ref, wu_ref, part_ref, ys):
    returned(meta[0], perm_t_ref[...], gg_ref, gu_ref, wg_ref, wu_ref, ys, part_ref)


def expert_back(meta, perm_t, gg, gu, wg, wu):
    return pl.pallas_call(
        back_kernel,
        name="expert_back",
        in_specs=whole(5),
        out_specs=pl.BlockSpec(memory_space=pltpu.VMEM),
        out_shape=jax.ShapeDtypeStruct((SLOTS, HALF // 2), BF),
        scratch_shapes=[pltpu.VMEM((2, ROWS, HALF // 2), BF)],
        compiler_params=vm(16),
        cost_estimate=cost(3e9),
    )(meta, perm_t, gg, gu, wg, wu)


def weight_kernel(
    meta, perm_ref, own_ref, peer_ref, hid_ref, gg_ref, gu_ref, og_ref, ou_ref, od_ref, xs, cs
):
    h = pl.program_id(1)
    perm = perm_ref[...]
    for g in range(8):
        rows = slice(g * GROUP, (g + 1) * GROUP)
        src = jnp.where(h == 0, own_ref[rows, :], peer_ref[rows, :])
        moved = dot(perm, src).astype(BF)
        xs[g * 96 : (g + 1) * 96, :] = moved[:96]
        cs[g * 96 : (g + 1) * 96, :] = moved[96:]
    x = xs[...]
    og_ref[...] = dot_rows(x, gg_ref[...])
    ou_ref[...] = dot_rows(x, gu_ref[...])
    od_ref[...] = dot_rows(hid_ref[...], cs[...])


def weight_grads(meta, perm, own, peer, hid, gg, gu):
    block = lambda j, h, m: 2 * j + (h + m[0]) % 2
    return pl.pallas_call(
        weight_kernel,
        name="weight_grads",
        grid_spec=pltpu.PrefetchScalarGridSpec(
            num_scalar_prefetch=1,
            grid=(4, 2),
            in_specs=[
                pl.BlockSpec((GROUP, GROUP), lambda j, h, m: (0, 0)),
                pl.BlockSpec((SLOTS, BLK), lambda j, h, m: (0, j)),
                pl.BlockSpec((SLOTS, BLK), lambda j, h, m: (0, j)),
                pl.BlockSpec((ROWS, FF), lambda j, h, m: (0, 0)),
                pl.BlockSpec((ROWS, FF), lambda j, h, m: (0, 0)),
                pl.BlockSpec((ROWS, FF), lambda j, h, m: (0, 0)),
            ],
            out_specs=[
                pl.BlockSpec((BLK, FF), lambda j, h, m: (block(j, h, m), 0)),
                pl.BlockSpec((BLK, FF), lambda j, h, m: (block(j, h, m), 0)),
                pl.BlockSpec((FF, BLK), lambda j, h, m: (0, block(j, h, m))),
            ],
            scratch_shapes=[pltpu.VMEM((ROWS, BLK), BF)] * 2,
        ),
        out_shape=[
            jax.ShapeDtypeStruct((D, FF), F32),
            jax.ShapeDtypeStruct((D, FF), F32),
            jax.ShapeDtypeStruct((FF, D), F32),
        ],
        compiler_params=vm(18),
        cost_estimate=pl.CostEstimate(
            flops=3 * 2 * ROWS * D * FF, bytes_accessed=20_000_000, transcendentals=0
        ),
    )(meta, perm, own, peer, hid, gg, gu)


def combine_kernel(
    meta, ids_hbm, ret_hbm, d_hbm, dm_ref, b0, b1, b2, b3, ids, ret, own, sems
):
    tp, z = meta[0], meta[1]
    cut = SLOTS // 4
    copies = fetch(
        [(ids_hbm, ids)]
        + [(ret_hbm.at[k * cut : (k + 1) * cut, :], ret.at[k * cut : (k + 1) * cut, :]) for k in range(4)]
        + [(d_hbm.at[:, lanes(2 * j + tp)], own.at[:, j * BLK : (j + 1) * BLK]) for j in range(4)],
        sems,
    )
    copies[0].wait()
    r0, r1 = slot_rows(ids)
    c0, c1 = as_column(r0).astype(jnp.int32), as_column(r1).astype(jnp.int32)
    low = high = 0.0
    for k in range(4):
        slot = lax.broadcasted_iota(jnp.int32, (TOK, cut), 1) + k * cut
        first = jnp.where((slot == c0) | (slot == c1), 1.0, 0.0).astype(BF)
        second = jnp.where((slot == c0 + CAP) | (slot == c1 + CAP), 1.0, 0.0).astype(BF)
        copies[1 + k].wait()
        piece = ret[k * cut : (k + 1) * cut, :]
        low += dot(first, piece)
        high += dot(second, piece)
    for copy in copies[5:]:
        copy.wait()
    dm_ref[:, :512] = (own[:, :512].astype(F32) + low).astype(BF)
    dm_ref[:, 512:] = (own[:, 512:].astype(F32) + high).astype(BF)
    for k, ref in enumerate((b0, b1, b2, b3)):
        ref[...] = dm_ref[:, lanes(lax.rem(z + k, 4))]


def combine(meta, ids, ret, d_out):
    return pl.pallas_call(
        combine_kernel,
        name="combine",
        in_specs=mixed("hhh"),
        out_specs=[pl.BlockSpec(memory_space=pltpu.VMEM)] * 5,
        out_shape=[jax.ShapeDtypeStruct((TOK, HALF), BF)]
        + [jax.ShapeDtypeStruct((TOK, BLK), BF)] * 4,
        scratch_shapes=[
            pltpu.VMEM((2, TOK), jnp.int32),
            pltpu.VMEM((SLOTS, HALF // 2), BF),
            pltpu.VMEM((TOK, HALF), BF),
            pltpu.SemaphoreType.DMA((9,)),
        ],
        compiler_params=vm(12),
        cost_estimate=cost(1e9),
    )(meta, *in_hbm(ids, ret, d_out))


ROOT = 0.7978845608028654
CUBE = 0.044715


def gelu_parts(x):
    t = jnp.tanh(ROOT * (x + CUBE * x * x * x))
    return 0.5 * x * (1.0 + t), t


def tile_of(line):
    return jnp.concatenate([line[:, k * 128 : (k + 1) * 128] for k in range(8)], axis=0)


def line_of(tile):
    return jnp.concatenate([tile[k : k + 1, :] for k in range(8)], axis=1)


def early_kernel(gate_ref, lru_ref, gated_ref):
    value, _ = gelu_parts(gate_ref[...].astype(F32))
    gated_ref[...] = (value * lru_ref[...].astype(F32)).astype(BF)


def early(gate_pre, lru_out):
    return pl.pallas_call(
        early_kernel,
        name="early",
        out_shape=jax.ShapeDtypeStruct((TOK, HALF), BF),
        compiler_params=vm(4),
        cost_estimate=cost(1e8),
    )(gate_pre, lru_out)


def scan_rows(drive_ref, rate_ref, start, visit):
    carry = start
    for tile in reversed(range(TOK // 8)):
        rows = slice(tile * 8, tile * 8 + 8)
        drive, rate = drive_ref[rows, :], rate_ref[rows, :]
        here, later = [None] * 8, [None] * 8
        for r in reversed(range(8)):
            here[r] = drive[r : r + 1] + carry
            carry = rate[r : r + 1] * here[r]
            later[r] = carry
        if visit is not None:
            visit(rows, jnp.concatenate(here, axis=0), jnp.concatenate(later, axis=0))
    return carry


def drive_kernel(
    meta, own_ref, peer_ref, w_hbm, gate_hbm, lru_hbm, decay_hbm,
    dgate_ref, drive_ref, head_ref, rate_ref, w, gate, lru, decay, sems,
):
    tp = meta[0]
    parts = [2 * j + tp for j in range(4)] + [2 * j + 1 - tp for j in range(4)]
    copies = fetch(
        [(w_hbm.at[:, lanes(part)], w.at[k, :, :]) for k, part in enumerate(parts)]
        + [(gate_hbm, gate), (lru_hbm, lru), (decay_hbm, decay)],
        sems,
    )
    grad = 0.0
    for k in range(8):
        copies[k].wait()
        ref, j = (own_ref, peer_ref)[k // 4], k % 4
        grad += dot_cols(ref[:, j * BLK : (j + 1) * BLK], w[k, :, :])
    for copy in copies[8:]:
        copy.wait()
    x = gate[...].astype(F32)
    value, t = gelu_parts(x)
    slope = 0.5 * (1.0 + t) + 0.5 * x * (1.0 - t * t) * (ROOT * (1.0 + 3.0 * CUBE * x * x))
    dgate_ref[...] = (grad * lru[...].astype(F32) * slope).astype(BF)
    drive_ref[...] = grad * value
    rate_ref[...] = jnp.exp(decay[...])
    head_ref[0:8, :] = tile_of(scan_rows(drive_ref, rate_ref, jnp.zeros((1, HALF), F32), None))
    head_ref[8:16, :] = tile_of(jnp.exp(jnp.sum(decay[...], axis=0, keepdims=True)))


def drive(meta, own, peer, w_out, gate_pre, lru_out, log_decay):
    return pl.pallas_call(
        drive_kernel,
        name="drive",
        in_specs=mixed("vvhhhh"),
        out_specs=[pl.BlockSpec(memory_space=pltpu.VMEM)] * 4,
        out_shape=[
            jax.ShapeDtypeStruct((TOK, HALF), BF),
            jax.ShapeDtypeStruct((TOK, HALF), F32),
            jax.ShapeDtypeStruct((16, 128), F32),
            jax.ShapeDtypeStruct((TOK, HALF), F32),
        ],
        scratch_shapes=[
            pltpu.VMEM((8, HALF, BLK), BF),
            pltpu.VMEM((TOK, HALF), BF),
            pltpu.VMEM((TOK, HALF), BF),
            pltpu.VMEM((TOK, HALF), F32),
            pltpu.SemaphoreType.DMA((11,)),
        ],
        compiler_params=vm(16),
        cost_estimate=cost(2e9),
    )(meta, own, peer, *in_hbm(w_out, gate_pre, lru_out, log_decay))


def link_kernel(meta, shares_ref, within_ref, after_ref, plane_ref):
    place = meta[3]
    within = jnp.zeros((8, 128), F32)
    total = jnp.zeros((8, 128), F32)
    after = jnp.ones((8, 128), F32)
    product = jnp.ones((8, 128), F32)
    for r in reversed(range(16)):
        tile = shares_ref[r, :, HALF:].astype(F32)
        head, block = tile[0:8] + tile[8:16], tile[16:24] + tile[24:32]
        total = head + block * total
        product = block * product
        within = jnp.where(place < r, total, within)
        after = jnp.where(place < r, product, after)
    within_ref[...] = within
    after_ref[...] = after
    plane_ref[0:8, :] = total
    plane_ref[8:16, :] = product


def link(meta, shares):
    return pl.pallas_call(
        link_kernel,
        name="link",
        in_specs=whole(1),
        out_specs=[pl.BlockSpec(memory_space=pltpu.VMEM)] * 3,
        out_shape=[
            jax.ShapeDtypeStruct((8, 128), F32),
            jax.ShapeDtypeStruct((8, 128), F32),
            jax.ShapeDtypeStruct((16, 128), F32),
        ],
        compiler_params=vm(8),
        cost_estimate=cost(1e7),
    )(meta, shares)


def finish_kernel(
    within_ref, after_ref, p1, p2, p3, drive_ref, rate_ref, lru_ref, before_ref, dd_ref, dl_ref,
    prev_ref,
):
    planes = p3[0:8, :]
    planes = p2[0:8, :] + p2[8:16, :] * planes
    planes = p1[0:8, :] + p1[8:16, :] * planes
    carry = line_of(within_ref[...] + after_ref[...] * planes)
    state = lru_ref[...].astype(F32)
    first = lax.broadcasted_iota(jnp.int32, (TOK, HALF), 0) == 0
    prev_ref[...] = jnp.where(first, before_ref[...].astype(F32), pltpu.roll(state, 1, 0))

    def visit(rows, here, later):
        dd_ref[rows, :] = here
        dl_ref[rows, :] = later * prev_ref[rows, :]

    scan_rows(drive_ref, rate_ref, carry, visit)


def finish(within, after, planes, drive_value, rate, lru_out, before):
    return pl.pallas_call(
        finish_kernel,
        name="finish",
        out_shape=[jax.ShapeDtypeStruct((TOK, HALF), F32)] * 2,
        scratch_shapes=[pltpu.VMEM((TOK, HALF), F32)],
        compiler_params=vm(8),
        cost_estimate=cost(1e8),
    )(within, after, *planes, drive_value, rate, lru_out, before)


def outer_own_kernel(b0, b1, b2, b3, g0, g1, g2, g3, out_ref, moved, sems):
    copies = fetch([(g, moved.at[k, :, :]) for k, g in enumerate((g0, g1, g2, g3))], sems)
    total = 0.0
    for k, ref in enumerate((b0, b1, b2, b3)):
        copies[k].wait()
        total += dot_rows(ref[...], moved[k, :, :])
    out_ref[...] = total.astype(BF)


def outer_own(blocks, gated):
    return pl.pallas_call(
        outer_own_kernel,
        name="outer_own",
        in_specs=mixed("vvvvhhhh")[1:],
        out_specs=pl.BlockSpec(memory_space=pltpu.VMEM),
        out_shape=jax.ShapeDtypeStruct((BLK, HALF), BF),
        scratch_shapes=[pltpu.VMEM((4, TOK, HALF), BF), pltpu.SemaphoreType.DMA((4,))],
        compiler_params=vm(10),
        cost_estimate=cost(1e9),
    )(*blocks, *in_hbm(*gated))


def outer_kernel(meta, p0, p1, p2, p3, g0, g1, g2, g3, own_ref, head_ref, out_ref, moved, sems):
    tp, z = meta[0], meta[1]
    copies = fetch([(g, moved.at[k, :, :]) for k, g in enumerate((g0, g1, g2, g3))], sems)
    out_ref[lanes(tp), 0:HALF] = own_ref[...]
    value = head_ref[...]
    high = value.astype(BF).astype(F32)
    low = value - high
    tile = jnp.concatenate([high[0:8], low[0:8], high[8:16], low[8:16]], axis=0).astype(BF)
    for k in range(16):
        out_ref[k * 32 : (k + 1) * 32, HALF:] = tile
    copies[0].wait()
    total = dot_rows(p0[:, lanes(z)], moved[0, :, :])
    for k, ref in ((1, p1), (2, p2), (3, p3)):
        copies[k].wait()
        total += dot_rows(ref[...], moved[k, :, :])
    out_ref[lanes(1 - tp), 0:HALF] = total.astype(BF)


def outer(meta, peer, gated, own, head):
    return pl.pallas_call(
        outer_kernel,
        name="outer",
        in_specs=mixed("vvvvhhhhvv"),
        out_specs=pl.BlockSpec(memory_space=pltpu.VMEM),
        out_shape=jax.ShapeDtypeStruct((2 * BLK, HALF + 128), BF),
        scratch_shapes=[pltpu.VMEM((4, TOK, HALF), BF), pltpu.SemaphoreType.DMA((4,))],
        compiler_params=vm(10),
        cost_estimate=cost(1e9),
    )(meta, *peer, *in_hbm(*gated), own, head)


def swapped(value):
    return lax.ppermute(value, "tp", [(0, 1), (1, 0)])


def turned(value, steps):
    return lax.ppermute(value, "z", [(s, (s + steps) % 4) for s in range(4)])


def on_device(
    stream_mid, d_out, route_ids, route_weights, gate_pre, lru_out, log_decay, w_out,
    exp_gate, exp_up, exp_down,
):
    meta = jnp.stack(
        [lax.axis_index("tp"), lax.axis_index("z"), lax.axis_index(SP), lax.axis_index(("y", "x"))]
    ).astype(jnp.int32)
    perm, perm_t = jnp.asarray(_perm, BF), jnp.asarray(_perm.T, BF)
    ids = route_ids.T
    wg, wu, wd = exp_gate[0], exp_up[0], exp_down[0]
    sent = pack(meta, ids, route_weights.T, stream_mid, d_out)
    got = lax.all_to_all(sent.reshape(NSP, CHUNK, HALF), SP, 0, 0, tiled=True)
    got = got.reshape(SLOTS, HALF)
    got_peer = swapped(got)
    gated = early(gate_pre, lru_out)
    gated, got = lax.optimization_barrier((gated, got))
    turn2 = turned(gated, 2)
    pg, pu, pb = expert_own(meta, perm, got, wg, wu, wd)
    hid, gg, gu, part_peer = expert_peer(meta, perm, perm_t, got_peer, wg, wu, wd, pg, pu, pb)
    other = swapped(part_peer)
    part_own = expert_back(meta, perm_t, gg, gu, wg, wu)
    back = part_sum(part_own, other)
    back, turn2 = lax.optimization_barrier((back, turn2))
    ret = lax.all_to_all(back.reshape(NSP, CHUNK, HALF // 2), SP, 0, 0, tiled=True)
    back, moving, last = lax.optimization_barrier((back, gated, lru_out[-1:]))
    turn1, turn3 = turned(moving, 1), turned(moving, 3)
    before = lax.ppermute(last, SP, [(s, s + 1) for s in range(NSP - 1)])
    grads = weight_grads(meta, perm, got, got_peer, hid, gg, gu)
    ret, grad_gate, grad_up, grad_down = lax.optimization_barrier((ret, *grads))
    dm, *blocks = combine(meta, ids, ret.reshape(SLOTS, HALF // 2), d_out)
    dm_peer = swapped(dm)
    own = (blocks[0], *(turned(blocks[k], k) for k in (1, 2, 3)))
    d_gate, drive_value, head, rate = drive(meta, dm, dm_peer, w_out, gate_pre, lru_out, log_decay)
    peer = (dm_peer, *(swapped(own[k]) for k in (1, 2, 3)))
    all_gated = (gated, turn1, turn2, turn3)
    share = outer(meta, peer, all_gated, outer_own(own, all_gated), head)
    shares = lax.all_to_all(share.reshape(16, 32, HALF + 128), ("y", "x"), 0, 0, tiled=True)
    within, after, plane = link(meta, shares)
    planes = [lax.ppermute(plane, "z", [(s, s - k) for s in range(k, 4)]) for k in (1, 2, 3)]
    d_drive, d_log_decay = finish(within, after, planes, drive_value, rate, lru_out, before)
    grad_out_proj = jnp.sum(shares[:, :, :HALF].astype(F32), axis=0)
    return (
        grad_gate[None], grad_up[None], grad_down[None], grad_out_proj, d_gate, d_drive, d_log_decay,
    )


def solution(mesh):
    fine = Mesh(mesh.devices.reshape(4, 4, 4, 2), ("z", "y", "x", "tp"))
    tokens = P(SP, None)
    both = P(SP, "tp")
    hidden = P(SP, None, "tp")
    in_specs = (
        tokens, tokens, tokens, tokens, both, both, both, P("tp", None),
        hidden, hidden, P(SP, "tp", None),
    )
    out_specs = (hidden, hidden, P(SP, "tp", None), both, both, both, both)
    return jax.shard_map(
        on_device, mesh=fine, in_specs=in_specs, out_specs=out_specs, check_vma=False
    )
```

```python
import jax
import jax.numpy as jnp
import numpy as np
from jax import lax
from jax.experimental import pallas as pl
from jax.experimental.pallas import tpu as pltpu
from jax.sharding import Mesh, PartitionSpec as P

BF = jnp.bfloat16
F32 = jnp.float32
SP = ("z", "y", "x")
TOK = 192
D = 2048
HALF = 1024
BLK = 256
CAP = 12
CHUNK = 24
NSP = 64
SLOTS = NSP * CHUNK
ROWS = NSP * CAP
FF = 512
GROUP = 8 * CHUNK

_perm = np.zeros((GROUP, GROUP), np.float32)
for _s in range(8):
    for _h in range(2):
        for _r in range(CAP):
            _perm[_h * 96 + _s * CAP + _r, _s * CHUNK + _h * CAP + _r] = 1.0


def dot(a, b):
    return lax.dot_general(a, b, (((1,), (0,)), ((), ())), preferred_element_type=F32)


def dot_cols(a, b):
    return lax.dot_general(a, b, (((1,), (1,)), ((), ())), preferred_element_type=F32)


def dot_rows(a, b):
    return lax.dot_general(a, b, (((0,), (0,)), ((), ())), preferred_element_type=F32)


def vm(mib):
    return pltpu.CompilerParams(vmem_limit_bytes=mib * 1024 * 1024)


def lanes(index, width=BLK):
    return pl.ds(pl.multiple_of(index * width, width), width)


def slot_rows(ids_ref):
    lane = lax.broadcasted_iota(jnp.int32, (NSP, TOK), 0)
    ids0, ids1 = ids_ref[0:1, :], ids_ref[1:2, :]
    hot0 = jnp.where(lane == ids0, 1.0, 0.0)
    hot1 = jnp.where(lane == ids1, 1.0, 0.0)
    row = lax.broadcasted_iota(jnp.int32, (TOK, TOK), 0)
    col = lax.broadcasted_iota(jnp.int32, (TOK, TOK), 1)
    before = jnp.where(row < col, 1.0, 0.0).astype(BF)
    rank0 = dot(hot0.astype(BF), before)
    rank1 = dot(hot1.astype(BF), before) + jnp.sum(hot0, axis=1, keepdims=True)
    first0 = jnp.sum(hot0 * rank0, axis=0, keepdims=True)
    first1 = jnp.sum(hot1 * rank1, axis=0, keepdims=True)
    return ids0.astype(F32) * CHUNK + first0, ids1.astype(F32) * CHUNK + first1


def as_column(line):
    row = lax.broadcasted_iota(jnp.int32, (TOK, TOK), 0)
    col = lax.broadcasted_iota(jnp.int32, (TOK, TOK), 1)
    return jnp.sum(jnp.where(row == col, line, 0.0), axis=1, keepdims=True)


def whole(count):
    vmem = pl.BlockSpec(memory_space=pltpu.VMEM)
    return [pl.BlockSpec(memory_space=pltpu.SMEM)] + [vmem] * count


def in_hbm(*values):
    return [pltpu.with_memory_space_constraint(v, pltpu.HBM) for v in values]


def mixed(*kinds):
    spaces = {"h": pltpu.HBM, "v": pltpu.VMEM, "a": pl.ANY}
    return [pl.BlockSpec(memory_space=pltpu.SMEM)] + [
        pl.BlockSpec(memory_space=spaces[k]) for k in "".join(kinds)
    ]


def fetch(pairs, sems):
    copies = [pltpu.make_async_copy(a, b, sems.at[k]) for k, (a, b) in enumerate(pairs)]
    for copy in copies:
        copy.start()
    return copies


def cost(flops, moved=0):
    return pl.CostEstimate(flops=int(flops), bytes_accessed=int(moved), transcendentals=0)


def pack_kernel(meta, ids_hbm, w_hbm, x_hbm, d_hbm, out_ref, ids, w, xs, ds, sems):
    tp = meta[0]
    small = [
        pltpu.make_async_copy(ids_hbm, ids, sems.at[0]),
        pltpu.make_async_copy(w_hbm, w, sems.at[1]),
    ]
    large = []
    for n, (src, dst) in enumerate(((x_hbm, xs), (d_hbm, ds))):
        for j in range(4):
            large.append(
                pltpu.make_async_copy(
                    src.at[:, lanes(2 * j + tp)],
                    dst.at[:, j * BLK : (j + 1) * BLK],
                    sems.at[2 + 4 * n + j],
                )
            )
    for copy in small + large:
        copy.start()
    for copy in small:
        copy.wait()
    r0, r1 = slot_rows(ids)
    r0, r1 = r0.astype(jnp.int32), r1.astype(jnp.int32)
    slot = lax.broadcasted_iota(jnp.int32, (SLOTS, TOK), 0)
    sx = jnp.where((slot == r0) | (slot == r1), 1.0, 0.0).astype(BF)
    s0 = jnp.where(slot == r0 + CAP, 1.0, 0.0).astype(BF)
    s1 = jnp.where(slot == r1 + CAP, 1.0, 0.0).astype(BF)
    w0, w1 = as_column(w[0:1, :]), as_column(w[1:2, :])
    for copy in large:
        copy.wait()
    for j in range(4):
        part = slice(j * BLK, (j + 1) * BLK)
        d = ds[:, part].astype(F32)
        scaled0, scaled1 = (w0 * d).astype(BF), (w1 * d).astype(BF)
        out = dot(sx, xs[:, part]) + dot(s0, scaled0) + dot(s1, scaled1)
        out_ref[:, part] = out.astype(BF)


def pack(meta, ids, weights, stream, d_out):
    hbm = pl.BlockSpec(memory_space=pltpu.HBM)
    return pl.pallas_call(
        pack_kernel,
        name="pack",
        in_specs=[pl.BlockSpec(memory_space=pltpu.SMEM)] + [hbm] * 4,
        out_specs=pl.BlockSpec(memory_space=pltpu.VMEM),
        out_shape=jax.ShapeDtypeStruct((SLOTS, HALF), BF),
        scratch_shapes=[
            pltpu.VMEM((2, TOK), jnp.int32),
            pltpu.VMEM((2, TOK), F32),
            pltpu.VMEM((TOK, HALF), BF),
            pltpu.VMEM((TOK, HALF), BF),
            pltpu.SemaphoreType.DMA((10,)),
        ],
        compiler_params=vm(12),
    )(meta, *in_hbm(ids, weights, stream, d_out))


def sum_kernel(a_ref, b_ref, out_hbm, both, sems):
    copies = []
    for k in range(4):
        rows = slice(k * 384, (k + 1) * 384)
        both[rows, :] = (a_ref[rows, :].astype(F32) + b_ref[rows, :].astype(F32)).astype(BF)
        copies.append(pltpu.make_async_copy(both.at[rows, :], out_hbm.at[rows, :], sems.at[k]))
        copies[-1].start()
    for copy in copies:
        copy.wait()


def part_sum(a, b):
    return pl.pallas_call(
        sum_kernel,
        name="part_sum",
        in_specs=[pl.BlockSpec(memory_space=pltpu.VMEM)] * 2,
        out_specs=pl.BlockSpec(memory_space=pltpu.HBM),
        out_shape=jax.ShapeDtypeStruct((SLOTS, HALF // 2), BF),
        scratch_shapes=[pltpu.VMEM((SLOTS, HALF // 2), BF), pltpu.SemaphoreType.DMA((4,))],
        compiler_params=vm(4),
    )(a, b)


def compact(perm, src_ref, xs, cs):
    for g in range(8):
        moved = dot(perm, src_ref[g * GROUP : (g + 1) * GROUP, :]).astype(BF)
        xs[g * 96 : (g + 1) * 96, :] = moved[:96]
        cs[g * 96 : (g + 1) * 96, :] = moved[96:]


def projections(par, xs, cs, wg_ref, wu_ref, wd_ref):
    gate = up = back = 0.0
    for j in range(4):
        mine, part = slice(j * BLK, (j + 1) * BLK), lanes(2 * j + par)
        gate += dot(xs[:, mine], wg_ref[part, :])
        up += dot(xs[:, mine], wu_ref[part, :])
        back += dot_cols(cs[:, mine], wd_ref[:, part])
    return gate, up, back


def returned(par, perm_t, gg_ref, gu_ref, wg_ref, wu_ref, ys, dst_ref):
    gg, gu = gg_ref[...], gu_ref[...]
    for j in range(4):
        part = lanes(2 * j + par)
        y = dot_cols(gg, wg_ref[part, :]) + dot_cols(gu, wu_ref[part, :])
        ys[j // 2, :, (j % 2) * BLK : (j % 2 + 1) * BLK] = y.astype(BF)
    for g in range(8):
        rows = slice(g * 96, (g + 1) * 96)
        both = jnp.concatenate([ys[0, rows, :], ys[1, rows, :]], axis=0)
        dst_ref[g * GROUP : (g + 1) * GROUP, :] = dot(perm_t, both).astype(BF)


def own_kernel(meta, perm_ref, own_ref, wg_ref, wu_ref, wd_ref, pg_ref, pu_ref, pb_ref, xs, cs):
    compact(perm_ref[...], own_ref, xs, cs)
    gate, up, back = projections(meta[0], xs, cs, wg_ref, wu_ref, wd_ref)
    pg_ref[...] = gate
    pu_ref[...] = up
    pb_ref[...] = back


def expert_own(meta, perm, own, wg, wu, wd):
    return pl.pallas_call(
        own_kernel,
        name="expert_own",
        in_specs=whole(5),
        out_specs=[pl.BlockSpec(memory_space=pltpu.VMEM)] * 3,
        out_shape=[jax.ShapeDtypeStruct((ROWS, FF), F32)] * 3,
        scratch_shapes=[pltpu.VMEM((ROWS, HALF), BF)] * 2,
        compiler_params=vm(16),
        cost_estimate=cost(4e9),
    )(meta, perm, own, wg, wu, wd)


def peer_kernel(
    meta, perm_ref, perm_t_ref, peer_ref, wg_ref, wu_ref, wd_ref, pg_ref, pu_ref, pb_ref,
    hid_ref, gg_ref, gu_ref, part_ref, xs, cs, ys,
):
    par = 1 - meta[0]
    compact(perm_ref[...], peer_ref, xs, cs)
    gate, up, back = projections(par, xs, cs, wg_ref, wu_ref, wd_ref)
    gate += pg_ref[...]
    up += pu_ref[...]
    back += pb_ref[...]
    sig = jax.nn.sigmoid(gate)
    act = gate * sig
    hid_ref[...] = (act * up).astype(BF)
    gg_ref[...] = (back * up * sig * (1.0 + gate * (1.0 - sig))).astype(BF)
    gu_ref[...] = (back * act).astype(BF)
    returned(par, perm_t_ref[...], gg_ref, gu_ref, wg_ref, wu_ref, ys, part_ref)


def expert_peer(meta, perm, perm_t, peer, wg, wu, wd, pg, pu, pb):
    return pl.pallas_call(
        peer_kernel,
        name="expert_peer",
        in_specs=whole(9),
        out_specs=[pl.BlockSpec(memory_space=pltpu.VMEM)] * 4,
        out_shape=[jax.ShapeDtypeStruct((ROWS, FF), BF)] * 3
        + [jax.ShapeDtypeStruct((SLOTS, HALF // 2), BF)],
        scratch_shapes=[pltpu.VMEM((ROWS, HALF), BF)] * 2 + [pltpu.VMEM((2, ROWS, HALF // 2), BF)],
        compiler_params=vm(20),
        cost_estimate=cost(6e9),
    )(meta, perm, perm_t, peer, wg, wu, wd, pg, pu, pb)


def back_kernel(meta, perm_t_ref, gg_ref, gu_ref, wg_ref, wu_ref, part_ref, ys):
    returned(meta[0], perm_t_ref[...], gg_ref, gu_ref, wg_ref, wu_ref, ys, part_ref)


def expert_back(meta, perm_t, gg, gu, wg, wu):
    return pl.pallas_call(
        back_kernel,
        name="expert_back",
        in_specs=whole(5),
        out_specs=pl.BlockSpec(memory_space=pltpu.VMEM),
        out_shape=jax.ShapeDtypeStruct((SLOTS, HALF // 2), BF),
        scratch_shapes=[pltpu.VMEM((2, ROWS, HALF // 2), BF)],
        compiler_params=vm(16),
        cost_estimate=cost(3e9),
    )(meta, perm_t, gg, gu, wg, wu)


def weight_kernel(
    meta, perm_ref, own_ref, peer_ref, hid_ref, gg_ref, gu_ref, og_ref, ou_ref, od_ref, xs, cs
):
    h = pl.program_id(1)
    perm = perm_ref[...]
    for g in range(8):
        rows = slice(g * GROUP, (g + 1) * GROUP)
        src = jnp.where(h == 0, own_ref[rows, :], peer_ref[rows, :])
        moved = dot(perm, src).astype(BF)
        xs[g * 96 : (g + 1) * 96, :] = moved[:96]
        cs[g * 96 : (g + 1) * 96, :] = moved[96:]
    x = xs[...]
    og_ref[...] = dot_rows(x, gg_ref[...])
    ou_ref[...] = dot_rows(x, gu_ref[...])
    od_ref[...] = dot_rows(hid_ref[...], cs[...])


def weight_grads(meta, perm, own, peer, hid, gg, gu):
    block = lambda j, h, m: 2 * j + (h + m[0]) % 2
    return pl.pallas_call(
        weight_kernel,
        name="weight_grads",
        grid_spec=pltpu.PrefetchScalarGridSpec(
            num_scalar_prefetch=1,
            grid=(4, 2),
            in_specs=[
                pl.BlockSpec((GROUP, GROUP), lambda j, h, m: (0, 0)),
                pl.BlockSpec((SLOTS, BLK), lambda j, h, m: (0, j)),
                pl.BlockSpec((SLOTS, BLK), lambda j, h, m: (0, j)),
                pl.BlockSpec((ROWS, FF), lambda j, h, m: (0, 0)),
                pl.BlockSpec((ROWS, FF), lambda j, h, m: (0, 0)),
                pl.BlockSpec((ROWS, FF), lambda j, h, m: (0, 0)),
            ],
            out_specs=[
                pl.BlockSpec((BLK, FF), lambda j, h, m: (block(j, h, m), 0)),
                pl.BlockSpec((BLK, FF), lambda j, h, m: (block(j, h, m), 0)),
                pl.BlockSpec((FF, BLK), lambda j, h, m: (0, block(j, h, m))),
            ],
            scratch_shapes=[pltpu.VMEM((ROWS, BLK), BF)] * 2,
        ),
        out_shape=[
            jax.ShapeDtypeStruct((D, FF), F32),
            jax.ShapeDtypeStruct((D, FF), F32),
            jax.ShapeDtypeStruct((FF, D), F32),
        ],
        compiler_params=vm(18),
        cost_estimate=pl.CostEstimate(
            flops=3 * 2 * ROWS * D * FF, bytes_accessed=20_000_000, transcendentals=0
        ),
    )(meta, *in_hbm(perm, own, peer, hid, gg, gu))


def combine_kernel(
    meta, ids_hbm, ret, d_hbm, w_hbm, dm_ref, b0, b1, b2, b3, w_ref, ids, own, sems
):
    tp, z = meta[0], meta[1]
    cut = SLOTS // 4
    copies = fetch(
        [(ids_hbm, ids)]
        + [(d_hbm.at[:, lanes(2 * j + tp)], own.at[:, j * BLK : (j + 1) * BLK]) for j in range(4)]
        + [(w_hbm.at[:, lanes(2 * j + tp)], w_ref.at[j, :, :]) for j in range(4)]
        + [(w_hbm.at[:, lanes(2 * j + 1 - tp)], w_ref.at[4 + j, :, :]) for j in range(4)],
        sems,
    )
    copies[0].wait()
    r0, r1 = slot_rows(ids)
    c0, c1 = as_column(r0).astype(jnp.int32), as_column(r1).astype(jnp.int32)
    low = high = 0.0
    for k in range(4):
        slot = lax.broadcasted_iota(jnp.int32, (TOK, cut), 1) + k * cut
        first = jnp.where((slot == c0) | (slot == c1), 1.0, 0.0).astype(BF)
        second = jnp.where((slot == c0 + CAP) | (slot == c1 + CAP), 1.0, 0.0).astype(BF)
        piece = ret[k * cut : (k + 1) * cut, :]
        low += dot(first, piece)
        high += dot(second, piece)
    for copy in copies[1:5]:
        copy.wait()
    dm_ref[:, :512] = (own[:, :512].astype(F32) + low).astype(BF)
    dm_ref[:, 512:] = (own[:, 512:].astype(F32) + high).astype(BF)
    for k, ref in enumerate((b0, b1, b2, b3)):
        ref[...] = dm_ref[:, lanes(lax.rem(z + k, 4))]
    for copy in copies[5:]:
        copy.wait()


def combine(meta, ids, ret, d_out, w_out):
    return pl.pallas_call(
        combine_kernel,
        name="combine",
        in_specs=mixed("hvhh"),
        out_specs=[pl.BlockSpec(memory_space=pltpu.VMEM)] * 6,
        out_shape=[jax.ShapeDtypeStruct((TOK, HALF), BF)]
        + [jax.ShapeDtypeStruct((TOK, BLK), BF)] * 4
        + [jax.ShapeDtypeStruct((8, HALF, BLK), BF)],
        scratch_shapes=[
            pltpu.VMEM((2, TOK), jnp.int32),
            pltpu.VMEM((TOK, HALF), BF),
            pltpu.SemaphoreType.DMA((13,)),
        ],
        compiler_params=vm(12),
        cost_estimate=cost(1e9),
    )(meta, *in_hbm(ids), ret, *in_hbm(d_out, w_out))


ROOT = 0.7978845608028654
CUBE = 0.044715


def gelu_parts(x):
    t = jnp.tanh(ROOT * (x + CUBE * x * x * x))
    return 0.5 * x * (1.0 + t), t


def tile_of(line):
    return jnp.concatenate([line[:, k * 128 : (k + 1) * 128] for k in range(8)], axis=0)


def line_of(tile):
    return jnp.concatenate([tile[k : k + 1, :] for k in range(8)], axis=1)


def early_kernel(gate_ref, lru_ref, gated_ref):
    value, _ = gelu_parts(gate_ref[...].astype(F32))
    gated_ref[...] = (value * lru_ref[...].astype(F32)).astype(BF)


def early(gate_pre, lru_out):
    return pl.pallas_call(
        early_kernel,
        name="early",
        out_shape=jax.ShapeDtypeStruct((TOK, HALF), BF),
        compiler_params=vm(4),
        cost_estimate=cost(1e8),
    )(gate_pre, lru_out)


def scan_rows(drive_ref, rate_ref, start, visit):
    carry = start
    for tile in reversed(range(TOK // 8)):
        rows = slice(tile * 8, tile * 8 + 8)
        drive, rate = drive_ref[rows, :], rate_ref[rows, :]
        here, later = [None] * 8, [None] * 8
        for r in reversed(range(8)):
            here[r] = drive[r : r + 1] + carry
            carry = rate[r : r + 1] * here[r]
            later[r] = carry
        if visit is not None:
            visit(rows, jnp.concatenate(here, axis=0), jnp.concatenate(later, axis=0))
    return carry


def prep_kernel(
    gate_hbm, lru_hbm, decay_hbm, before_ref, value_hbm, slope_hbm, rate_hbm, after_hbm, past_hbm,
    gate, lru, decay, value, slope, rate, after, past, sems,
):
    for copy in fetch([(gate_hbm, gate), (lru_hbm, lru), (decay_hbm, decay)], sems):
        copy.wait()
    x = gate[...].astype(F32)
    state = lru[...].astype(F32)
    gelu, t = gelu_parts(x)
    value[...] = gelu
    out0 = fetch([(value, value_hbm)], sems.at[3:4])
    grown = 0.5 * (1.0 + t) + 0.5 * x * (1.0 - t * t) * (ROOT * (1.0 + 3.0 * CUBE * x * x))
    slope[...] = grown * state
    out1 = fetch([(slope, slope_hbm)], sems.at[4:5])
    rate[...] = jnp.exp(decay[...])
    first = lax.broadcasted_iota(jnp.int32, (TOK, HALF), 0) == 0
    prev = jnp.where(first, before_ref[...].astype(F32), pltpu.roll(state, 1, 0))
    past[...] = rate[...] * prev
    out2 = fetch([(rate, rate_hbm), (past, past_hbm)], sems.at[5:7])
    carry = jnp.ones((1, HALF), F32)
    for tile in reversed(range(TOK // 8)):
        rows = slice(tile * 8, tile * 8 + 8)
        decays, here = rate[rows, :], [None] * 8
        for r in reversed(range(8)):
            here[r] = carry
            carry = decays[r : r + 1] * carry
        after[rows, :] = jnp.concatenate(here, axis=0)
    for copy in out0 + out1 + out2 + fetch([(after, after_hbm)], sems.at[7:8]):
        copy.wait()


def prep(gate_pre, lru_out, log_decay, before):
    bf, wide = pltpu.VMEM((TOK, HALF), BF), pltpu.VMEM((TOK, HALF), F32)
    return pl.pallas_call(
        prep_kernel,
        name="prep",
        in_specs=mixed("hhhv")[1:],
        out_specs=[pl.BlockSpec(memory_space=pltpu.HBM)] * 5,
        out_shape=[pltpu.HBM((TOK, HALF), F32)] * 5,
        scratch_shapes=[bf, bf] + [wide] * 6 + [pltpu.SemaphoreType.DMA((8,))],
        compiler_params=vm(12),
        cost_estimate=cost(1e9),
    )(*in_hbm(gate_pre, lru_out, log_decay), before)


def drive_kernel(
    meta, own_ref, peer_ref, w_ref, value_hbm, slope_hbm, rate_hbm, after_hbm, g0, g1, g2, g3,
    dgate_ref, local_ref, head_ref, moved_ref, value, slope, rate, after, sems,
):
    copies = fetch(
        [
            (value_hbm, value),
            (slope_hbm, slope),
            (rate_hbm, rate),
            (after_hbm.at[0:8, :], after),
            (g0, moved_ref.at[0, :, :]),
            (g1, moved_ref.at[1, :, :]),
            (g2, moved_ref.at[2, :, :]),
            (g3, moved_ref.at[3, :, :]),
        ],
        sems,
    )
    grad = 0.0
    for k in range(8):
        ref, j = (own_ref, peer_ref)[k // 4], k % 4
        grad += dot_cols(ref[:, j * BLK : (j + 1) * BLK], w_ref[k, :, :])
    copies[0].wait()
    local_ref[...] = grad * value[...]
    copies[1].wait()
    dgate_ref[...] = (grad * slope[...]).astype(BF)
    copies[2].wait()
    copies[3].wait()

    def visit(rows, here, later):
        local_ref[rows, :] = here

    head_ref[0:8, :] = tile_of(scan_rows(local_ref, rate, jnp.zeros((1, HALF), F32), visit))
    head_ref[8:16, :] = tile_of(after[0:1, :] * rate[0:1, :])
    for copy in copies[4:]:
        copy.wait()


def drive(meta, own, peer, w, value, slope, rate, after, gated):
    wide = pltpu.VMEM((TOK, HALF), F32)
    return pl.pallas_call(
        drive_kernel,
        name="drive",
        in_specs=mixed("vvvhhhhaaaa"),
        out_specs=[pl.BlockSpec(memory_space=pltpu.VMEM)] * 4,
        out_shape=[
            jax.ShapeDtypeStruct((TOK, HALF), BF),
            jax.ShapeDtypeStruct((TOK, HALF), F32),
            jax.ShapeDtypeStruct((16, 128), F32),
            jax.ShapeDtypeStruct((4, TOK, HALF), BF),
        ],
        scratch_shapes=[wide, wide, wide, pltpu.VMEM((8, HALF), F32), pltpu.SemaphoreType.DMA((8,))],
        compiler_params=vm(12),
        cost_estimate=cost(2e9),
    )(meta, own, peer, w, *in_hbm(value, slope, rate, after), *gated)


def link_kernel(meta, shares_ref, within_ref, after_ref, plane_ref):
    place = meta[3]
    within = jnp.zeros((8, 128), F32)
    total = jnp.zeros((8, 128), F32)
    after = jnp.ones((8, 128), F32)
    product = jnp.ones((8, 128), F32)
    for r in reversed(range(16)):
        tile = shares_ref[r, :, HALF:].astype(F32)
        head, block = tile[0:8] + tile[8:16], tile[16:24] + tile[24:32]
        total = head + block * total
        product = block * product
        within = jnp.where(place < r, total, within)
        after = jnp.where(place < r, product, after)
    within_ref[...] = within
    after_ref[...] = after
    plane_ref[0:8, :] = total
    plane_ref[8:16, :] = product


def link(meta, shares):
    return pl.pallas_call(
        link_kernel,
        name="link",
        in_specs=whole(1),
        out_specs=[pl.BlockSpec(memory_space=pltpu.VMEM)] * 3,
        out_shape=[
            jax.ShapeDtypeStruct((8, 128), F32),
            jax.ShapeDtypeStruct((8, 128), F32),
            jax.ShapeDtypeStruct((16, 128), F32),
        ],
        compiler_params=vm(8),
        cost_estimate=cost(1e7),
    )(meta, shares)


def finish_kernel(within_ref, after_ref, p1, p2, p3, local_ref, suffix_ref, past_ref, dd_ref, dl_ref):
    planes = p3[0:8, :]
    planes = p2[0:8, :] + p2[8:16, :] * planes
    planes = p1[0:8, :] + p1[8:16, :] * planes
    incoming = line_of(within_ref[...] + after_ref[...] * planes)
    for tile in range(TOK // 8):
        rows = slice(tile * 8, tile * 8 + 8)
        value = local_ref[rows, :] + suffix_ref[rows, :] * incoming
        dd_ref[rows, :] = value
        dl_ref[rows, :] = value * past_ref[rows, :]


def finish(within, after, planes, local, suffix, past):
    return pl.pallas_call(
        finish_kernel,
        name="finish",
        out_shape=[jax.ShapeDtypeStruct((TOK, HALF), F32)] * 2,
        compiler_params=vm(8),
        cost_estimate=cost(1e9),
    )(within, after, *planes, local, suffix, past)


def outer_own_kernel(b0, b1, b2, b3, moved, out_ref):
    total = 0.0
    for k, ref in enumerate((b0, b1, b2, b3)):
        total += dot_rows(ref[...], moved[k, :, :])
    out_ref[...] = total.astype(BF)


def outer_own(blocks, moved):
    return pl.pallas_call(
        outer_own_kernel,
        name="outer_own",
        in_specs=mixed("vvvvv")[1:],
        out_specs=pl.BlockSpec(memory_space=pltpu.VMEM),
        out_shape=jax.ShapeDtypeStruct((BLK, HALF), BF),
        compiler_params=vm(8),
        cost_estimate=cost(1e9),
    )(*blocks, moved)


def outer_kernel(meta, p0, p1, p2, p3, moved, own_ref, head_ref, out_ref):
    tp, z = meta[0], meta[1]
    out_ref[lanes(tp), 0:HALF] = own_ref[...]
    value = head_ref[...]
    high = value.astype(BF).astype(F32)
    low = value - high
    tile = jnp.concatenate([high[0:8], low[0:8], high[8:16], low[8:16]], axis=0).astype(BF)
    for k in range(16):
        out_ref[k * 32 : (k + 1) * 32, HALF:] = tile
    total = dot_rows(p0[:, lanes(z)], moved[0, :, :])
    for k, ref in ((1, p1), (2, p2), (3, p3)):
        total += dot_rows(ref[...], moved[k, :, :])
    out_ref[lanes(1 - tp), 0:HALF] = total.astype(BF)


def outer(meta, peer, moved, own, head):
    return pl.pallas_call(
        outer_kernel,
        name="outer",
        in_specs=mixed("vvvvvvv"),
        out_specs=pl.BlockSpec(memory_space=pltpu.VMEM),
        out_shape=jax.ShapeDtypeStruct((2 * BLK, HALF + 128), BF),
        compiler_params=vm(8),
        cost_estimate=cost(1e9),
    )(meta, *peer, moved, own, head)


def swapped(value):
    return lax.ppermute(value, "tp", [(0, 1), (1, 0)])


def turned(value, steps):
    return lax.ppermute(value, "z", [(s, (s + steps) % 4) for s in range(4)])


def on_device(
    stream_mid, d_out, route_ids, route_weights, gate_pre, lru_out, log_decay, w_out,
    exp_gate, exp_up, exp_down,
):
    meta = jnp.stack(
        [lax.axis_index("tp"), lax.axis_index("z"), lax.axis_index(SP), lax.axis_index(("y", "x"))]
    ).astype(jnp.int32)
    perm, perm_t = jnp.asarray(_perm, BF), jnp.asarray(_perm.T, BF)
    ids = route_ids.T
    wg, wu, wd = exp_gate[0], exp_up[0], exp_down[0]
    sent = pack(meta, ids, route_weights.T, stream_mid, d_out)
    got = lax.all_to_all(sent.reshape(NSP, CHUNK, HALF), SP, 0, 0, tiled=True)
    got = got.reshape(SLOTS, HALF)
    got_peer = swapped(got)
    gated = early(gate_pre, lru_out)
    gated, got = lax.optimization_barrier((gated, got))
    turn2 = turned(gated, 2)
    pg, pu, pb = expert_own(meta, perm, got, wg, wu, wd)
    hid, gg, gu, part_peer = expert_peer(meta, perm, perm_t, got_peer, wg, wu, wd, pg, pu, pb)
    other = swapped(part_peer)
    part_own = expert_back(meta, perm_t, gg, gu, wg, wu)
    back = part_sum(part_own, other)
    back, turn2 = lax.optimization_barrier((back, turn2))
    ret = lax.all_to_all(back.reshape(NSP, CHUNK, HALF // 2), SP, 0, 0, tiled=True)
    back, moving, last = lax.optimization_barrier((back, gated, lru_out[-1:]))
    turn1, turn3 = turned(moving, 1), turned(moving, 3)
    before = lax.ppermute(last, SP, [(s, s + 1) for s in range(NSP - 1)])
    value, slope, rate, suffix, past = prep(gate_pre, lru_out, log_decay, before)
    grads = weight_grads(meta, perm, got, got_peer, hid, gg, gu)
    ret, rate, grad_gate, grad_up, grad_down = lax.optimization_barrier((ret, rate, *grads))
    dm, *blocks, w = combine(meta, ids, ret.reshape(SLOTS, HALF // 2), d_out, w_out)
    dm_peer = swapped(dm)
    own = (blocks[0], *(turned(blocks[k], k) for k in (1, 2, 3)))
    d_gate, local, head, moved = drive(
        meta, dm, dm_peer, w, value, slope, rate, suffix, (gated, turn1, turn2, turn3)
    )
    peer = (dm_peer, *(swapped(own[k]) for k in (1, 2, 3)))
    share = outer(meta, peer, moved, outer_own(own, moved), head)
    shares = lax.all_to_all(share.reshape(16, 32, HALF + 128), ("y", "x"), 0, 0, tiled=True)
    within, after, plane = link(meta, shares)
    planes = [lax.ppermute(plane, "z", [(s, s - k) for s in range(k, 4)]) for k in (1, 2, 3)]
    d_drive, d_log_decay = finish(within, after, planes, local, suffix, past)
    grad_out_proj = jnp.sum(shares[:, :, :HALF].astype(F32), axis=0)
    return (
        grad_gate[None], grad_up[None], grad_down[None], grad_out_proj, d_gate, d_drive, d_log_decay,
    )


def solution(mesh):
    fine = Mesh(mesh.devices.reshape(4, 4, 4, 2), ("z", "y", "x", "tp"))
    tokens = P(SP, None)
    both = P(SP, "tp")
    hidden = P(SP, None, "tp")
    in_specs = (
        tokens, tokens, tokens, tokens, both, both, both, P("tp", None),
        hidden, hidden, P(SP, "tp", None),
    )
    out_specs = (hidden, hidden, P(SP, "tp", None), both, both, both, both)
    return jax.shard_map(
        on_device, mesh=fine, in_specs=in_specs, out_specs=out_specs, check_vma=False
    )
```

```python
import jax
import jax.numpy as jnp
import numpy as np
from jax import lax
from jax.experimental import pallas as pl
from jax.experimental.pallas import tpu as pltpu
from jax.sharding import Mesh, PartitionSpec as P

BF = jnp.bfloat16
F32 = jnp.float32
SP = ("z", "y", "x")
TOK = 192
D = 2048
HALF = 1024
BLK = 256
CAP = 12
CHUNK = 24
NSP = 64
SLOTS = NSP * CHUNK
ROWS = NSP * CAP
FF = 512
STRIP = 24
GROUP = 8 * CHUNK

_perm = np.zeros((GROUP, GROUP), np.float32)
for _s in range(8):
    for _h in range(2):
        for _r in range(CAP):
            _perm[_h * 96 + _s * CAP + _r, _s * CHUNK + _h * CAP + _r] = 1.0


def dot(a, b):
    return lax.dot_general(a, b, (((1,), (0,)), ((), ())), preferred_element_type=F32)


def dot_cols(a, b):
    return lax.dot_general(a, b, (((1,), (1,)), ((), ())), preferred_element_type=F32)


def dot_rows(a, b):
    return lax.dot_general(a, b, (((0,), (0,)), ((), ())), preferred_element_type=F32)


def vm(mib):
    return pltpu.CompilerParams(vmem_limit_bytes=mib * 1024 * 1024)


def lanes(index, width=BLK):
    return pl.ds(pl.multiple_of(index * width, width), width)


def slot_rows(ids_ref):
    lane = lax.broadcasted_iota(jnp.int32, (NSP, TOK), 0)
    ids0, ids1 = ids_ref[0:1, :], ids_ref[1:2, :]
    hot0 = jnp.where(lane == ids0, 1.0, 0.0)
    hot1 = jnp.where(lane == ids1, 1.0, 0.0)
    row = lax.broadcasted_iota(jnp.int32, (TOK, TOK), 0)
    col = lax.broadcasted_iota(jnp.int32, (TOK, TOK), 1)
    before = jnp.where(row < col, 1.0, 0.0).astype(BF)
    rank0 = dot(hot0.astype(BF), before)
    rank1 = dot(hot1.astype(BF), before) + jnp.sum(hot0, axis=1, keepdims=True)
    first0 = jnp.sum(hot0 * rank0, axis=0, keepdims=True)
    first1 = jnp.sum(hot1 * rank1, axis=0, keepdims=True)
    return ids0.astype(F32) * CHUNK + first0, ids1.astype(F32) * CHUNK + first1


def as_column(line):
    row = lax.broadcasted_iota(jnp.int32, (TOK, TOK), 0)
    col = lax.broadcasted_iota(jnp.int32, (TOK, TOK), 1)
    return jnp.sum(jnp.where(row == col, line, 0.0), axis=1, keepdims=True)


def whole(count):
    vmem = pl.BlockSpec(memory_space=pltpu.VMEM)
    return [pl.BlockSpec(memory_space=pltpu.SMEM)] + [vmem] * count


def in_hbm(*values):
    return [pltpu.with_memory_space_constraint(v, pltpu.HBM) for v in values]


def mixed(*kinds):
    spaces = {"h": pltpu.HBM, "v": pltpu.VMEM, "a": pl.ANY}
    return [pl.BlockSpec(memory_space=pltpu.SMEM)] + [
        pl.BlockSpec(memory_space=spaces[k]) for k in "".join(kinds)
    ]


def fetch(pairs, sems):
    copies = [pltpu.make_async_copy(a, b, sems.at[k]) for k, (a, b) in enumerate(pairs)]
    for copy in copies:
        copy.start()
    return copies


def cost(flops, moved=0):
    return pl.CostEstimate(flops=int(flops), bytes_accessed=int(moved), transcendentals=0)


def pack_kernel(meta, ids_hbm, w_hbm, x_hbm, d_hbm, out_ref, ids, w, xs, ds, sems):
    tp = meta[0]
    small = [
        pltpu.make_async_copy(ids_hbm, ids, sems.at[0]),
        pltpu.make_async_copy(w_hbm, w, sems.at[1]),
    ]
    large = []
    for n, (src, dst) in enumerate(((x_hbm, xs), (d_hbm, ds))):
        for j in range(4):
            large.append(
                pltpu.make_async_copy(
                    src.at[:, lanes(2 * j + tp)],
                    dst.at[:, j * BLK : (j + 1) * BLK],
                    sems.at[2 + 4 * n + j],
                )
            )
    for copy in small + large:
        copy.start()
    for copy in small:
        copy.wait()
    r0, r1 = slot_rows(ids)
    r0, r1 = r0.astype(jnp.int32), r1.astype(jnp.int32)
    slot = lax.broadcasted_iota(jnp.int32, (SLOTS, TOK), 0)
    sx = jnp.where((slot == r0) | (slot == r1), 1.0, 0.0).astype(BF)
    s0 = jnp.where(slot == r0 + CAP, 1.0, 0.0).astype(BF)
    s1 = jnp.where(slot == r1 + CAP, 1.0, 0.0).astype(BF)
    w0, w1 = as_column(w[0:1, :]), as_column(w[1:2, :])
    for copy in large:
        copy.wait()
    for j in range(4):
        part = slice(j * BLK, (j + 1) * BLK)
        d = ds[:, part].astype(F32)
        scaled0, scaled1 = (w0 * d).astype(BF), (w1 * d).astype(BF)
        out = dot(sx, xs[:, part]) + dot(s0, scaled0) + dot(s1, scaled1)
        out_ref[:, part] = out.astype(BF)


def pack(meta, ids, weights, stream, d_out):
    hbm = pl.BlockSpec(memory_space=pltpu.HBM)
    return pl.pallas_call(
        pack_kernel,
        name="pack",
        in_specs=[pl.BlockSpec(memory_space=pltpu.SMEM)] + [hbm] * 4,
        out_specs=pl.BlockSpec(memory_space=pltpu.VMEM),
        out_shape=jax.ShapeDtypeStruct((SLOTS, HALF), BF),
        scratch_shapes=[
            pltpu.VMEM((2, TOK), jnp.int32),
            pltpu.VMEM((2, TOK), F32),
            pltpu.VMEM((TOK, HALF), BF),
            pltpu.VMEM((TOK, HALF), BF),
            pltpu.SemaphoreType.DMA((10,)),
        ],
        compiler_params=vm(12),
    )(meta, *in_hbm(ids, weights, stream, d_out))


def sum_kernel(a_ref, b_ref, out_hbm, both, sems):
    copies = []
    for k in range(4):
        rows = slice(k * 384, (k + 1) * 384)
        both[rows, :] = (a_ref[rows, :].astype(F32) + b_ref[rows, :].astype(F32)).astype(BF)
        copies.append(pltpu.make_async_copy(both.at[rows, :], out_hbm.at[rows, :], sems.at[k]))
        copies[-1].start()
    for copy in copies:
        copy.wait()


def part_sum(a, b):
    return pl.pallas_call(
        sum_kernel,
        name="part_sum",
        in_specs=[pl.BlockSpec(memory_space=pltpu.VMEM)] * 2,
        out_specs=pl.BlockSpec(memory_space=pltpu.HBM),
        out_shape=jax.ShapeDtypeStruct((SLOTS, HALF // 2), BF),
        scratch_shapes=[pltpu.VMEM((SLOTS, HALF // 2), BF), pltpu.SemaphoreType.DMA((4,))],
        compiler_params=vm(4),
    )(a, b)


def compact(perm, src_ref, xs, cs):
    for g in range(8):
        moved = dot(perm, src_ref[g * GROUP : (g + 1) * GROUP, :]).astype(BF)
        xs[g * 96 : (g + 1) * 96, :] = moved[:96]
        cs[g * 96 : (g + 1) * 96, :] = moved[96:]


def projections(par, xs, cs, wg_ref, wu_ref, wd_ref):
    gate = up = back = 0.0
    for j in range(4):
        mine, part = slice(j * BLK, (j + 1) * BLK), lanes(2 * j + par)
        gate += dot(xs[:, mine], wg_ref[part, :])
        up += dot(xs[:, mine], wu_ref[part, :])
        back += dot_cols(cs[:, mine], wd_ref[:, part])
    return gate, up, back


def returned(par, perm_t, gg_ref, gu_ref, wg_ref, wu_ref, ys, dst_ref):
    gg, gu = gg_ref[...], gu_ref[...]
    for j in range(4):
        part = lanes(2 * j + par)
        y = dot_cols(gg, wg_ref[part, :]) + dot_cols(gu, wu_ref[part, :])
        ys[j // 2, :, (j % 2) * BLK : (j % 2 + 1) * BLK] = y.astype(BF)
    for g in range(8):
        rows = slice(g * 96, (g + 1) * 96)
        both = jnp.concatenate([ys[0, rows, :], ys[1, rows, :]], axis=0)
        dst_ref[g * GROUP : (g + 1) * GROUP, :] = dot(perm_t, both).astype(BF)


def own_kernel(meta, perm_ref, own_ref, wg_ref, wu_ref, wd_ref, pg_ref, pu_ref, pb_ref, xs, cs):
    compact(perm_ref[...], own_ref, xs, cs)
    gate, up, back = projections(meta[0], xs, cs, wg_ref, wu_ref, wd_ref)
    pg_ref[...] = gate
    pu_ref[...] = up
    pb_ref[...] = back


def expert_own(meta, perm, own, wg, wu, wd):
    return pl.pallas_call(
        own_kernel,
        name="expert_own",
        in_specs=whole(5),
        out_specs=[pl.BlockSpec(memory_space=pltpu.VMEM)] * 3,
        out_shape=[jax.ShapeDtypeStruct((ROWS, FF), F32)] * 3,
        scratch_shapes=[pltpu.VMEM((ROWS, HALF), BF)] * 2,
        compiler_params=vm(16),
        cost_estimate=cost(4e9),
    )(meta, perm, own, wg, wu, wd)


def peer_kernel(
    meta, perm_ref, perm_t_ref, peer_ref, wg_ref, wu_ref, wd_ref, pg_ref, pu_ref, pb_ref,
    hid_ref, gg_ref, gu_ref, part_ref, xs, cs, ys,
):
    par = 1 - meta[0]
    compact(perm_ref[...], peer_ref, xs, cs)
    gate, up, back = projections(par, xs, cs, wg_ref, wu_ref, wd_ref)
    gate += pg_ref[...]
    up += pu_ref[...]
    back += pb_ref[...]
    sig = jax.nn.sigmoid(gate)
    act = gate * sig
    hid_ref[...] = (act * up).astype(BF)
    gg_ref[...] = (back * up * sig * (1.0 + gate * (1.0 - sig))).astype(BF)
    gu_ref[...] = (back * act).astype(BF)
    returned(par, perm_t_ref[...], gg_ref, gu_ref, wg_ref, wu_ref, ys, part_ref)


def expert_peer(meta, perm, perm_t, peer, wg, wu, wd, pg, pu, pb):
    return pl.pallas_call(
        peer_kernel,
        name="expert_peer",
        in_specs=whole(9),
        out_specs=[pl.BlockSpec(memory_space=pltpu.VMEM)] * 4,
        out_shape=[jax.ShapeDtypeStruct((ROWS, FF), BF)] * 3
        + [jax.ShapeDtypeStruct((SLOTS, HALF // 2), BF)],
        scratch_shapes=[pltpu.VMEM((ROWS, HALF), BF)] * 2 + [pltpu.VMEM((2, ROWS, HALF // 2), BF)],
        compiler_params=vm(20),
        cost_estimate=cost(6e9),
    )(meta, perm, perm_t, peer, wg, wu, wd, pg, pu, pb)


def back_kernel(meta, perm_t_ref, gg_ref, gu_ref, wg_ref, wu_ref, part_ref, ys):
    returned(meta[0], perm_t_ref[...], gg_ref, gu_ref, wg_ref, wu_ref, ys, part_ref)


def expert_back(meta, perm_t, gg, gu, wg, wu):
    return pl.pallas_call(
        back_kernel,
        name="expert_back",
        in_specs=whole(5),
        out_specs=pl.BlockSpec(memory_space=pltpu.VMEM),
        out_shape=jax.ShapeDtypeStruct((SLOTS, HALF // 2), BF),
        scratch_shapes=[pltpu.VMEM((2, ROWS, HALF // 2), BF)],
        compiler_params=vm(16),
        cost_estimate=cost(3e9),
    )(meta, perm_t, gg, gu, wg, wu)


ROOT = 0.7978845608028654
CUBE = 0.044715


def gelu_parts(x):
    t = jnp.tanh(ROOT * (x + CUBE * x * x * x))
    return 0.5 * x * (1.0 + t), t


def weight_kernel(
    meta, perm_ref, own_ref, peer_ref, hid_ref, gg_ref, gu_ref, gate_ref, lru_ref, decay_ref,
    og_ref, ou_ref, od_ref, value_ref, slope_ref, rate_ref, after_ref, xs, cs, carry_ref,
):
    j, h = pl.program_id(0), pl.program_id(1)

    @pl.when((j == 0) & (h == 0))
    def _():
        carry_ref[...] = jnp.ones((1, HALF), F32)

    v = gate_ref[...].astype(F32)
    value, t = gelu_parts(v)
    value_ref[...] = value
    grown = 0.5 * (1.0 + t) + 0.5 * v * (1.0 - t * t) * (ROOT * (1.0 + 3.0 * CUBE * v * v))
    slope_ref[...] = grown * lru_ref[...].astype(F32)
    rate_ref[...] = jnp.exp(decay_ref[...])
    carry = carry_ref[...]
    for tile in reversed(range(STRIP // 8)):
        rows = slice(tile * 8, tile * 8 + 8)
        decays, here = rate_ref[rows, :], [None] * 8
        for r in reversed(range(8)):
            here[r] = carry
            carry = decays[r : r + 1] * carry
        after_ref[rows, :] = jnp.concatenate(here, axis=0)
    carry_ref[...] = carry
    perm = perm_ref[...]
    for g in range(8):
        rows = slice(g * GROUP, (g + 1) * GROUP)
        src = jnp.where(h == 0, own_ref[rows, :], peer_ref[rows, :])
        moved = dot(perm, src).astype(BF)
        xs[g * 96 : (g + 1) * 96, :] = moved[:96]
        cs[g * 96 : (g + 1) * 96, :] = moved[96:]
    x = xs[...]
    og_ref[...] = dot_rows(x, gg_ref[...])
    ou_ref[...] = dot_rows(x, gu_ref[...])
    od_ref[...] = dot_rows(hid_ref[...], cs[...])


def weight_grads(meta, perm, own, peer, hid, gg, gu, gate_pre, lru_out, log_decay):
    strip = pl.BlockSpec((STRIP, HALF), lambda j, h, m: (7 - 2 * j - h, 0))
    block = lambda j, h, m: 2 * j + (h + m[0]) % 2
    return pl.pallas_call(
        weight_kernel,
        name="weight_grads",
        grid_spec=pltpu.PrefetchScalarGridSpec(
            num_scalar_prefetch=1,
            grid=(4, 2),
            in_specs=[
                pl.BlockSpec((GROUP, GROUP), lambda j, h, m: (0, 0)),
                pl.BlockSpec((SLOTS, BLK), lambda j, h, m: (0, j)),
                pl.BlockSpec((SLOTS, BLK), lambda j, h, m: (0, j)),
                pl.BlockSpec((ROWS, FF), lambda j, h, m: (0, 0)),
                pl.BlockSpec((ROWS, FF), lambda j, h, m: (0, 0)),
                pl.BlockSpec((ROWS, FF), lambda j, h, m: (0, 0)),
            ]
            + [strip] * 3,
            out_specs=[
                pl.BlockSpec((BLK, FF), lambda j, h, m: (block(j, h, m), 0)),
                pl.BlockSpec((BLK, FF), lambda j, h, m: (block(j, h, m), 0)),
                pl.BlockSpec((FF, BLK), lambda j, h, m: (0, block(j, h, m))),
            ]
            + [strip] * 4,
            scratch_shapes=[pltpu.VMEM((ROWS, BLK), BF)] * 2 + [pltpu.VMEM((1, HALF), F32)],
        ),
        out_shape=[
            jax.ShapeDtypeStruct((D, FF), F32),
            jax.ShapeDtypeStruct((D, FF), F32),
            jax.ShapeDtypeStruct((FF, D), F32),
        ]
        + [pltpu.HBM((TOK, HALF), F32)] * 4,
        compiler_params=vm(18),
        cost_estimate=pl.CostEstimate(
            flops=3 * 2 * ROWS * D * FF, bytes_accessed=20_000_000, transcendentals=0
        ),
    )(meta, *in_hbm(perm, own, peer, hid, gg, gu, gate_pre, lru_out, log_decay))


def combine_kernel(
    meta, ids_hbm, ret, d_hbm, w_hbm, dm_ref, b0, b1, b2, b3, w_ref, ids, own, sems
):
    tp, z = meta[0], meta[1]
    cut = SLOTS // 4
    copies = fetch(
        [(ids_hbm, ids)]
        + [(d_hbm.at[:, lanes(2 * j + tp)], own.at[:, j * BLK : (j + 1) * BLK]) for j in range(4)]
        + [(w_hbm.at[:, lanes(2 * j + tp)], w_ref.at[j, :, :]) for j in range(4)],
        sems,
    )
    copies[0].wait()
    r0, r1 = slot_rows(ids)
    c0, c1 = as_column(r0).astype(jnp.int32), as_column(r1).astype(jnp.int32)
    low = high = 0.0
    for k in range(4):
        slot = lax.broadcasted_iota(jnp.int32, (TOK, cut), 1) + k * cut
        first = jnp.where((slot == c0) | (slot == c1), 1.0, 0.0).astype(BF)
        second = jnp.where((slot == c0 + CAP) | (slot == c1 + CAP), 1.0, 0.0).astype(BF)
        piece = ret[k * cut : (k + 1) * cut, :]
        low += dot(first, piece)
        high += dot(second, piece)
    for copy in copies[1:5]:
        copy.wait()
    dm_ref[:, :512] = (own[:, :512].astype(F32) + low).astype(BF)
    dm_ref[:, 512:] = (own[:, 512:].astype(F32) + high).astype(BF)
    for k, ref in enumerate((b0, b1, b2, b3)):
        ref[...] = dm_ref[:, lanes(lax.rem(z + k, 4))]
    for copy in copies[5:]:
        copy.wait()


def combine(meta, ids, ret, d_out, w_out):
    return pl.pallas_call(
        combine_kernel,
        name="combine",
        in_specs=mixed("hvhh"),
        out_specs=[pl.BlockSpec(memory_space=pltpu.VMEM)] * 6,
        out_shape=[jax.ShapeDtypeStruct((TOK, HALF), BF)]
        + [jax.ShapeDtypeStruct((TOK, BLK), BF)] * 4
        + [jax.ShapeDtypeStruct((4, HALF, BLK), BF)],
        scratch_shapes=[
            pltpu.VMEM((2, TOK), jnp.int32),
            pltpu.VMEM((TOK, HALF), BF),
            pltpu.SemaphoreType.DMA((9,)),
        ],
        compiler_params=vm(12),
        cost_estimate=cost(1e9),
    )(meta, *in_hbm(ids), ret, *in_hbm(d_out, w_out))


def tile_of(line):
    return jnp.concatenate([line[:, k * 128 : (k + 1) * 128] for k in range(8)], axis=0)


def line_of(tile):
    return jnp.concatenate([tile[k : k + 1, :] for k in range(8)], axis=1)


def early_kernel(gate_ref, lru_ref, gated_ref):
    value, _ = gelu_parts(gate_ref[...].astype(F32))
    gated_ref[...] = (value * lru_ref[...].astype(F32)).astype(BF)


def early(gate_pre, lru_out):
    return pl.pallas_call(
        early_kernel,
        name="early",
        out_shape=jax.ShapeDtypeStruct((TOK, HALF), BF),
        compiler_params=vm(4),
        cost_estimate=cost(1e8),
    )(gate_pre, lru_out)


def scan_rows(drive_ref, rate_ref, start, visit):
    carry = start
    for tile in reversed(range(TOK // 8)):
        rows = slice(tile * 8, tile * 8 + 8)
        drive, rate = drive_ref[rows, :], rate_ref[rows, :]
        here, later = [None] * 8, [None] * 8
        for r in reversed(range(8)):
            here[r] = drive[r : r + 1] + carry
            carry = rate[r : r + 1] * here[r]
            later[r] = carry
        if visit is not None:
            visit(rows, jnp.concatenate(here, axis=0), jnp.concatenate(later, axis=0))
    return carry


def drive_kernel(
    meta, own_ref, peer_ref, w_ref, w_hbm, value_hbm, slope_hbm, rate_hbm, after_hbm, g0, g1, g2, g3,
    dgate_ref, local_ref, head_ref, moved_ref, w, value, slope, rate, after, sems,
):
    tp = meta[0]
    copies = fetch(
        [(w_hbm.at[:, lanes(2 * j + 1 - tp)], w.at[j, :, :]) for j in range(4)]
        + [
            (value_hbm, value),
            (rate_hbm, rate),
            (after_hbm.at[0:8, :], after),
            (slope_hbm, slope),
        ],
        sems,
    )
    grad = 0.0
    for j in range(4):
        grad += dot_cols(own_ref[:, j * BLK : (j + 1) * BLK], w_ref[j, :, :])
    for j in range(4):
        copies[j].wait()
        grad += dot_cols(peer_ref[:, j * BLK : (j + 1) * BLK], w[j, :, :])
    copies[4].wait()
    local_ref[...] = grad * value[...]
    for copy in copies[5:]:
        copy.wait()
    late = fetch([(g, moved_ref.at[k, :, :]) for k, g in enumerate((g0, g1, g2, g3))], sems.at[8:12])
    dgate_ref[...] = (grad * slope[...]).astype(BF)

    def visit(rows, here, later):
        local_ref[rows, :] = here

    head_ref[0:8, :] = tile_of(scan_rows(local_ref, rate, jnp.zeros((1, HALF), F32), visit))
    head_ref[8:16, :] = tile_of(after[0:1, :] * rate[0:1, :])
    for copy in late:
        copy.wait()


def drive(meta, own, peer, w, w_out, value, slope, rate, after, gated):
    wide = pltpu.VMEM((TOK, HALF), F32)
    return pl.pallas_call(
        drive_kernel,
        name="drive",
        in_specs=mixed("vvvhhhhhaaaa"),
        out_specs=[pl.BlockSpec(memory_space=pltpu.VMEM)] * 4,
        out_shape=[
            jax.ShapeDtypeStruct((TOK, HALF), BF),
            jax.ShapeDtypeStruct((TOK, HALF), F32),
            jax.ShapeDtypeStruct((16, 128), F32),
            jax.ShapeDtypeStruct((4, TOK, HALF), BF),
        ],
        scratch_shapes=[pltpu.VMEM((4, HALF, BLK), BF), wide, wide, wide]
        + [pltpu.VMEM((8, HALF), F32), pltpu.SemaphoreType.DMA((12,))],
        compiler_params=vm(12),
        cost_estimate=cost(2e9),
    )(meta, own, peer, w, *in_hbm(w_out, value, slope, rate, after), *gated)


def link_kernel(meta, shares_ref, within_ref, after_ref, plane_ref):
    place = meta[3]
    within = jnp.zeros((8, 128), F32)
    total = jnp.zeros((8, 128), F32)
    after = jnp.ones((8, 128), F32)
    product = jnp.ones((8, 128), F32)
    for r in reversed(range(16)):
        tile = shares_ref[r, :, HALF:].astype(F32)
        head, block = tile[0:8] + tile[8:16], tile[16:24] + tile[24:32]
        total = head + block * total
        product = block * product
        within = jnp.where(place < r, total, within)
        after = jnp.where(place < r, product, after)
    within_ref[...] = within
    after_ref[...] = after
    plane_ref[0:8, :] = total
    plane_ref[8:16, :] = product


def link(meta, shares):
    return pl.pallas_call(
        link_kernel,
        name="link",
        in_specs=whole(1),
        out_specs=[pl.BlockSpec(memory_space=pltpu.VMEM)] * 3,
        out_shape=[
            jax.ShapeDtypeStruct((8, 128), F32),
            jax.ShapeDtypeStruct((8, 128), F32),
            jax.ShapeDtypeStruct((16, 128), F32),
        ],
        compiler_params=vm(8),
        cost_estimate=cost(1e7),
    )(meta, shares)


def finish_kernel(
    within_ref, after_ref, p1, p2, p3, local_ref, suffix_ref, rate_ref, lru_ref, before_ref,
    dd_ref, dl_ref,
):
    planes = p3[0:8, :]
    planes = p2[0:8, :] + p2[8:16, :] * planes
    planes = p1[0:8, :] + p1[8:16, :] * planes
    incoming = line_of(within_ref[...] + after_ref[...] * planes)
    value = local_ref[...] + suffix_ref[...] * incoming
    dd_ref[...] = value
    first = lax.broadcasted_iota(jnp.int32, (TOK, HALF), 0) == 0
    state = pltpu.roll(lru_ref[...].astype(F32), 1, 0)
    dl_ref[...] = value * rate_ref[...] * jnp.where(first, before_ref[...].astype(F32), state)


def finish(within, after, planes, local, suffix, rate, lru_out, before):
    return pl.pallas_call(
        finish_kernel,
        name="finish",
        out_shape=[jax.ShapeDtypeStruct((TOK, HALF), F32)] * 2,
        compiler_params=vm(8),
        cost_estimate=cost(1e9),
    )(within, after, *planes, local, suffix, rate, lru_out, before)


def outer_own_kernel(b0, b1, b2, b3, moved, out_ref):
    total = 0.0
    for k, ref in enumerate((b0, b1, b2, b3)):
        total += dot_rows(ref[...], moved[k, :, :])
    out_ref[...] = total.astype(BF)


def outer_own(blocks, moved):
    return pl.pallas_call(
        outer_own_kernel,
        name="outer_own",
        in_specs=mixed("vvvvv")[1:],
        out_specs=pl.BlockSpec(memory_space=pltpu.VMEM),
        out_shape=jax.ShapeDtypeStruct((BLK, HALF), BF),
        compiler_params=vm(8),
        cost_estimate=cost(1e9),
    )(*blocks, moved)


def outer_kernel(meta, p0, p1, p2, p3, moved, own_ref, head_ref, out_ref):
    tp, z = meta[0], meta[1]
    out_ref[lanes(tp), 0:HALF] = own_ref[...]
    value = head_ref[...]
    high = value.astype(BF).astype(F32)
    low = value - high
    tile = jnp.concatenate([high[0:8], low[0:8], high[8:16], low[8:16]], axis=0).astype(BF)
    for k in range(16):
        out_ref[k * 32 : (k + 1) * 32, HALF:] = tile
    total = dot_rows(p0[:, lanes(z)], moved[0, :, :])
    for k, ref in ((1, p1), (2, p2), (3, p3)):
        total += dot_rows(ref[...], moved[k, :, :])
    out_ref[lanes(1 - tp), 0:HALF] = total.astype(BF)


def outer(meta, peer, moved, own, head):
    return pl.pallas_call(
        outer_kernel,
        name="outer",
        in_specs=mixed("vvvvvvv"),
        out_specs=pl.BlockSpec(memory_space=pltpu.VMEM),
        out_shape=jax.ShapeDtypeStruct((2 * BLK, HALF + 128), BF),
        compiler_params=vm(8),
        cost_estimate=cost(1e9),
    )(meta, *peer, moved, own, head)


def swapped(value):
    return lax.ppermute(value, "tp", [(0, 1), (1, 0)])


def turned(value, steps):
    return lax.ppermute(value, "z", [(s, (s + steps) % 4) for s in range(4)])


def on_device(
    stream_mid, d_out, route_ids, route_weights, gate_pre, lru_out, log_decay, w_out,
    exp_gate, exp_up, exp_down,
):
    meta = jnp.stack(
        [lax.axis_index("tp"), lax.axis_index("z"), lax.axis_index(SP), lax.axis_index(("y", "x"))]
    ).astype(jnp.int32)
    perm, perm_t = jnp.asarray(_perm, BF), jnp.asarray(_perm.T, BF)
    ids = route_ids.T
    wg, wu, wd = exp_gate[0], exp_up[0], exp_down[0]
    sent = pack(meta, ids, route_weights.T, stream_mid, d_out)
    got = lax.all_to_all(sent.reshape(NSP, CHUNK, HALF), SP, 0, 0, tiled=True)
    got = got.reshape(SLOTS, HALF)
    got_peer = swapped(got)
    gated = early(gate_pre, lru_out)
    gated, got = lax.optimization_barrier((gated, got))
    turn2 = turned(gated, 2)
    pg, pu, pb = expert_own(meta, perm, got, wg, wu, wd)
    hid, gg, gu, part_peer = expert_peer(meta, perm, perm_t, got_peer, wg, wu, wd, pg, pu, pb)
    other = swapped(part_peer)
    part_own = expert_back(meta, perm_t, gg, gu, wg, wu)
    back = part_sum(part_own, other)
    back, turn2 = lax.optimization_barrier((back, turn2))
    ret = lax.all_to_all(back.reshape(NSP, CHUNK, HALF // 2), SP, 0, 0, tiled=True)
    back, moving, last = lax.optimization_barrier((back, gated, lru_out[-1:]))
    turn1, turn3 = turned(moving, 1), turned(moving, 3)
    before = lax.ppermute(last, SP, [(s, s + 1) for s in range(NSP - 1)])
    grads = weight_grads(
        meta, perm, got, got_peer, hid, gg, gu, gate_pre, lru_out, log_decay
    )
    ret, *grads = lax.optimization_barrier((ret, *grads))
    grad_gate, grad_up, grad_down, value, slope, rate, suffix = grads
    dm, *blocks, w = combine(meta, ids, ret.reshape(SLOTS, HALF // 2), d_out, w_out)
    dm_peer = swapped(dm)
    own = (blocks[0], *(turned(blocks[k], k) for k in (1, 2, 3)))
    d_gate, local, head, moved = drive(
        meta, dm, dm_peer, w, w_out, value, slope, rate, suffix, (gated, turn1, turn2, turn3)
    )
    peer = (dm_peer, *(swapped(own[k]) for k in (1, 2, 3)))
    share = outer(meta, peer, moved, outer_own(own, moved), head)
    shares = lax.all_to_all(share.reshape(16, 32, HALF + 128), ("y", "x"), 0, 0, tiled=True)
    within, after, plane = link(meta, shares)
    planes = [lax.ppermute(plane, "z", [(s, s - k) for s in range(k, 4)]) for k in (1, 2, 3)]
    d_drive, d_log_decay = finish(
        within, after, planes, local, suffix, rate, lru_out, before
    )
    grad_out_proj = jnp.sum(shares[:, :, :HALF].astype(F32), axis=0)
    return (
        grad_gate[None], grad_up[None], grad_down[None], grad_out_proj, d_gate, d_drive, d_log_decay,
    )


def solution(mesh):
    fine = Mesh(mesh.devices.reshape(4, 4, 4, 2), ("z", "y", "x", "tp"))
    tokens = P(SP, None)
    both = P(SP, "tp")
    hidden = P(SP, None, "tp")
    in_specs = (
        tokens, tokens, tokens, tokens, both, both, both, P("tp", None),
        hidden, hidden, P(SP, "tp", None),
    )
    out_specs = (hidden, hidden, P(SP, "tp", None), both, both, both, both)
    return jax.shard_map(
        on_device, mesh=fine, in_specs=in_specs, out_specs=out_specs, check_vma=False
    )
```

```python
import jax
import jax.numpy as jnp
import numpy as np
from jax import lax
from jax.experimental import pallas as pl
from jax.experimental.pallas import tpu as pltpu
from jax.sharding import Mesh, PartitionSpec as P

BF = jnp.bfloat16
F32 = jnp.float32
SP = ("z", "y", "x")
TOK = 192
D = 2048
HALF = 1024
BLK = 256
CAP = 12
CHUNK = 24
NSP = 64
SLOTS = NSP * CHUNK
ROWS = NSP * CAP
FF = 512
STRIP = 24
GROUP = 8 * CHUNK

_perm = np.zeros((GROUP, GROUP), np.float32)
for _s in range(8):
    for _h in range(2):
        for _r in range(CAP):
            _perm[_h * 96 + _s * CAP + _r, _s * CHUNK + _h * CAP + _r] = 1.0


def dot(a, b):
    return lax.dot_general(a, b, (((1,), (0,)), ((), ())), preferred_element_type=F32)


def dot_cols(a, b):
    return lax.dot_general(a, b, (((1,), (1,)), ((), ())), preferred_element_type=F32)


def dot_rows(a, b):
    return lax.dot_general(a, b, (((0,), (0,)), ((), ())), preferred_element_type=F32)


def vm(mib):
    return pltpu.CompilerParams(vmem_limit_bytes=mib * 1024 * 1024)


def lanes(index, width=BLK):
    return pl.ds(pl.multiple_of(index * width, width), width)


def slot_rows(ids_ref):
    lane = lax.broadcasted_iota(jnp.int32, (NSP, TOK), 0)
    ids0, ids1 = ids_ref[0:1, :], ids_ref[1:2, :]
    hot0 = jnp.where(lane == ids0, 1.0, 0.0)
    hot1 = jnp.where(lane == ids1, 1.0, 0.0)
    row = lax.broadcasted_iota(jnp.int32, (TOK, TOK), 0)
    col = lax.broadcasted_iota(jnp.int32, (TOK, TOK), 1)
    before = jnp.where(row < col, 1.0, 0.0).astype(BF)
    rank0 = dot(hot0.astype(BF), before)
    rank1 = dot(hot1.astype(BF), before) + jnp.sum(hot0, axis=1, keepdims=True)
    first0 = jnp.sum(hot0 * rank0, axis=0, keepdims=True)
    first1 = jnp.sum(hot1 * rank1, axis=0, keepdims=True)
    return ids0.astype(F32) * CHUNK + first0, ids1.astype(F32) * CHUNK + first1


def as_column(line):
    row = lax.broadcasted_iota(jnp.int32, (TOK, TOK), 0)
    col = lax.broadcasted_iota(jnp.int32, (TOK, TOK), 1)
    return jnp.sum(jnp.where(row == col, line, 0.0), axis=1, keepdims=True)


def whole(count):
    vmem = pl.BlockSpec(memory_space=pltpu.VMEM)
    return [pl.BlockSpec(memory_space=pltpu.SMEM)] + [vmem] * count


def in_hbm(*values):
    return [pltpu.with_memory_space_constraint(v, pltpu.HBM) for v in values]


def mixed(*kinds):
    spaces = {"h": pltpu.HBM, "v": pltpu.VMEM, "a": pl.ANY}
    return [pl.BlockSpec(memory_space=pltpu.SMEM)] + [
        pl.BlockSpec(memory_space=spaces[k]) for k in "".join(kinds)
    ]


def fetch(pairs, sems):
    copies = [pltpu.make_async_copy(a, b, sems.at[k]) for k, (a, b) in enumerate(pairs)]
    for copy in copies:
        copy.start()
    return copies


def cost(flops, moved=0):
    return pl.CostEstimate(flops=int(flops), bytes_accessed=int(moved), transcendentals=0)


def pack_kernel(meta, ids_hbm, w_hbm, x_hbm, d_hbm, out_ref, ids, w, xs, ds, sems):
    tp = meta[0]
    small = [
        pltpu.make_async_copy(ids_hbm, ids, sems.at[0]),
        pltpu.make_async_copy(w_hbm, w, sems.at[1]),
    ]
    large = []
    for n, (src, dst) in enumerate(((x_hbm, xs), (d_hbm, ds))):
        for j in range(4):
            large.append(
                pltpu.make_async_copy(
                    src.at[:, lanes(2 * j + tp)],
                    dst.at[:, j * BLK : (j + 1) * BLK],
                    sems.at[2 + 4 * n + j],
                )
            )
    for copy in small + large:
        copy.start()
    for copy in small:
        copy.wait()
    r0, r1 = slot_rows(ids)
    r0, r1 = r0.astype(jnp.int32), r1.astype(jnp.int32)
    slot = lax.broadcasted_iota(jnp.int32, (SLOTS, TOK), 0)
    sx = jnp.where((slot == r0) | (slot == r1), 1.0, 0.0).astype(BF)
    s0 = jnp.where(slot == r0 + CAP, 1.0, 0.0).astype(BF)
    s1 = jnp.where(slot == r1 + CAP, 1.0, 0.0).astype(BF)
    w0, w1 = as_column(w[0:1, :]), as_column(w[1:2, :])
    for copy in large:
        copy.wait()
    for j in range(4):
        part = slice(j * BLK, (j + 1) * BLK)
        d = ds[:, part].astype(F32)
        scaled0, scaled1 = (w0 * d).astype(BF), (w1 * d).astype(BF)
        out = dot(sx, xs[:, part]) + dot(s0, scaled0) + dot(s1, scaled1)
        out_ref[:, part] = out.astype(BF)


def pack(meta, ids, weights, stream, d_out):
    hbm = pl.BlockSpec(memory_space=pltpu.HBM)
    return pl.pallas_call(
        pack_kernel,
        name="pack",
        in_specs=[pl.BlockSpec(memory_space=pltpu.SMEM)] + [hbm] * 4,
        out_specs=pl.BlockSpec(memory_space=pltpu.VMEM),
        out_shape=jax.ShapeDtypeStruct((SLOTS, HALF), BF),
        scratch_shapes=[
            pltpu.VMEM((2, TOK), jnp.int32),
            pltpu.VMEM((2, TOK), F32),
            pltpu.VMEM((TOK, HALF), BF),
            pltpu.VMEM((TOK, HALF), BF),
            pltpu.SemaphoreType.DMA((10,)),
        ],
        compiler_params=vm(12),
    )(meta, *in_hbm(ids, weights, stream, d_out))


def sum_kernel(a_ref, b_ref, out_hbm, both, sems):
    copies = []
    for k in range(4):
        rows = slice(k * 384, (k + 1) * 384)
        both[rows, :] = (a_ref[rows, :].astype(F32) + b_ref[rows, :].astype(F32)).astype(BF)
        copies.append(pltpu.make_async_copy(both.at[rows, :], out_hbm.at[rows, :], sems.at[k]))
        copies[-1].start()
    for copy in copies:
        copy.wait()


def part_sum(a, b):
    return pl.pallas_call(
        sum_kernel,
        name="part_sum",
        in_specs=[pl.BlockSpec(memory_space=pltpu.VMEM)] * 2,
        out_specs=pl.BlockSpec(memory_space=pltpu.HBM),
        out_shape=jax.ShapeDtypeStruct((SLOTS, HALF // 2), BF),
        scratch_shapes=[pltpu.VMEM((SLOTS, HALF // 2), BF), pltpu.SemaphoreType.DMA((4,))],
        compiler_params=vm(4),
    )(a, b)


def compact(perm, src_ref, xs, cs):
    for g in range(8):
        moved = dot(perm, src_ref[g * GROUP : (g + 1) * GROUP, :]).astype(BF)
        xs[g * 96 : (g + 1) * 96, :] = moved[:96]
        cs[g * 96 : (g + 1) * 96, :] = moved[96:]


def projections(par, xs, cs, wg_ref, wu_ref, wd_ref, units=slice(None)):
    gate = up = back = 0.0
    for j in range(4):
        mine, part = slice(j * BLK, (j + 1) * BLK), lanes(2 * j + par)
        gate += dot(xs[:, mine], wg_ref[part, units])
        up += dot(xs[:, mine], wu_ref[part, units])
        back += dot_cols(cs[:, mine], wd_ref[units, part])
    return gate, up, back


def returned(par, perm_t, gg_ref, gu_ref, wg_ref, wu_ref, ys, dst_ref):
    gg, gu = gg_ref[...], gu_ref[...]
    for j in range(4):
        part = lanes(2 * j + par)
        y = dot_cols(gg, wg_ref[part, :]) + dot_cols(gu, wu_ref[part, :])
        ys[j // 2, :, (j % 2) * BLK : (j % 2 + 1) * BLK] = y.astype(BF)
    for g in range(8):
        rows = slice(g * 96, (g + 1) * 96)
        both = jnp.concatenate([ys[0, rows, :], ys[1, rows, :]], axis=0)
        dst_ref[g * GROUP : (g + 1) * GROUP, :] = dot(perm_t, both).astype(BF)


def own_kernel(meta, perm_ref, own_ref, wg_ref, wu_ref, wd_ref, pg_ref, pu_ref, pb_ref, xs, cs):
    compact(perm_ref[...], own_ref, xs, cs)
    gate, up, back = projections(meta[0], xs, cs, wg_ref, wu_ref, wd_ref)
    pg_ref[...] = gate
    pu_ref[...] = up
    pb_ref[...] = back


def expert_own(meta, perm, own, wg, wu, wd):
    return pl.pallas_call(
        own_kernel,
        name="expert_own",
        in_specs=whole(5),
        out_specs=[pl.BlockSpec(memory_space=pltpu.VMEM)] * 3,
        out_shape=[jax.ShapeDtypeStruct((ROWS, FF), F32)] * 3,
        scratch_shapes=[pltpu.VMEM((ROWS, HALF), BF)] * 2,
        compiler_params=vm(16),
        cost_estimate=cost(4e9),
    )(meta, perm, own, wg, wu, wd)


def peer_kernel(
    meta, perm_ref, perm_t_ref, peer_ref, wg_ref, wu_ref, wd_ref, pg_ref, pu_ref, pb_ref,
    hid_ref, gg_ref, gu_ref, part_ref, xs, cs, ys,
):
    par = 1 - meta[0]
    compact(perm_ref[...], peer_ref, xs, cs)
    for half in range(2):
        units = slice(half * BLK, (half + 1) * BLK)
        gate, up, back = projections(par, xs, cs, wg_ref, wu_ref, wd_ref, units)
        gate += pg_ref[:, units]
        up += pu_ref[:, units]
        back += pb_ref[:, units]
        sig = jax.nn.sigmoid(gate)
        act = gate * sig
        hid_ref[:, units] = (act * up).astype(BF)
        gg_ref[:, units] = (back * up * sig * (1.0 + gate * (1.0 - sig))).astype(BF)
        gu_ref[:, units] = (back * act).astype(BF)
    returned(par, perm_t_ref[...], gg_ref, gu_ref, wg_ref, wu_ref, ys, part_ref)


def expert_peer(meta, perm, perm_t, peer, wg, wu, wd, pg, pu, pb):
    return pl.pallas_call(
        peer_kernel,
        name="expert_peer",
        in_specs=whole(9),
        out_specs=[pl.BlockSpec(memory_space=pltpu.VMEM)] * 4,
        out_shape=[jax.ShapeDtypeStruct((ROWS, FF), BF)] * 3
        + [jax.ShapeDtypeStruct((SLOTS, HALF // 2), BF)],
        scratch_shapes=[pltpu.VMEM((ROWS, HALF), BF)] * 2 + [pltpu.VMEM((2, ROWS, HALF // 2), BF)],
        compiler_params=vm(20),
        cost_estimate=cost(6e9),
    )(meta, perm, perm_t, peer, wg, wu, wd, pg, pu, pb)


def back_kernel(meta, perm_t_ref, gg_ref, gu_ref, wg_ref, wu_ref, part_ref, ys):
    returned(meta[0], perm_t_ref[...], gg_ref, gu_ref, wg_ref, wu_ref, ys, part_ref)


def expert_back(meta, perm_t, gg, gu, wg, wu):
    return pl.pallas_call(
        back_kernel,
        name="expert_back",
        in_specs=whole(5),
        out_specs=pl.BlockSpec(memory_space=pltpu.VMEM),
        out_shape=jax.ShapeDtypeStruct((SLOTS, HALF // 2), BF),
        scratch_shapes=[pltpu.VMEM((2, ROWS, HALF // 2), BF)],
        compiler_params=vm(16),
        cost_estimate=cost(3e9),
    )(meta, perm_t, gg, gu, wg, wu)


ROOT = 0.7978845608028654
CUBE = 0.044715


def gelu_parts(x):
    t = jnp.tanh(ROOT * (x + CUBE * x * x * x))
    return 0.5 * x * (1.0 + t), t


def weight_kernel(
    meta, perm_ref, own_ref, peer_ref, hid_ref, gg_ref, gu_ref, gate_ref, lru_ref, decay_ref,
    og_ref, ou_ref, od_ref, value_ref, slope_ref, rate_ref, after_ref, xs, cs, carry_ref,
):
    j, h = pl.program_id(0), pl.program_id(1)

    @pl.when((j == 0) & (h == 0))
    def _():
        carry_ref[...] = jnp.ones((1, HALF), F32)

    v = gate_ref[...].astype(F32)
    value, t = gelu_parts(v)
    value_ref[...] = value
    grown = 0.5 * (1.0 + t) + 0.5 * v * (1.0 - t * t) * (ROOT * (1.0 + 3.0 * CUBE * v * v))
    slope_ref[...] = grown * lru_ref[...].astype(F32)
    rate_ref[...] = jnp.exp(decay_ref[...])
    carry = carry_ref[...]
    for tile in reversed(range(STRIP // 8)):
        rows = slice(tile * 8, tile * 8 + 8)
        decays, here = rate_ref[rows, :], [None] * 8
        for r in reversed(range(8)):
            here[r] = carry
            carry = decays[r : r + 1] * carry
        after_ref[rows, :] = jnp.concatenate(here, axis=0)
    carry_ref[...] = carry
    perm = perm_ref[...]
    for g in range(8):
        rows = slice(g * GROUP, (g + 1) * GROUP)
        src = jnp.where(h == 0, own_ref[rows, :], peer_ref[rows, :])
        moved = dot(perm, src).astype(BF)
        xs[g * 96 : (g + 1) * 96, :] = moved[:96]
        cs[g * 96 : (g + 1) * 96, :] = moved[96:]
    x = xs[...]
    og_ref[...] = dot_rows(x, gg_ref[...])
    ou_ref[...] = dot_rows(x, gu_ref[...])
    od_ref[...] = dot_rows(hid_ref[...], cs[...])


def weight_grads(meta, perm, own, peer, hid, gg, gu, gate_pre, lru_out, log_decay):
    strip = pl.BlockSpec((STRIP, HALF), lambda j, h, m: (7 - 2 * j - h, 0))
    block = lambda j, h, m: 2 * j + (h + m[0]) % 2
    return pl.pallas_call(
        weight_kernel,
        name="weight_grads",
        grid_spec=pltpu.PrefetchScalarGridSpec(
            num_scalar_prefetch=1,
            grid=(4, 2),
            in_specs=[
                pl.BlockSpec((GROUP, GROUP), lambda j, h, m: (0, 0)),
                pl.BlockSpec((SLOTS, BLK), lambda j, h, m: (0, j)),
                pl.BlockSpec((SLOTS, BLK), lambda j, h, m: (0, j)),
                pl.BlockSpec((ROWS, FF), lambda j, h, m: (0, 0)),
                pl.BlockSpec((ROWS, FF), lambda j, h, m: (0, 0)),
                pl.BlockSpec((ROWS, FF), lambda j, h, m: (0, 0)),
            ]
            + [strip] * 3,
            out_specs=[
                pl.BlockSpec((BLK, FF), lambda j, h, m: (block(j, h, m), 0)),
                pl.BlockSpec((BLK, FF), lambda j, h, m: (block(j, h, m), 0)),
                pl.BlockSpec((FF, BLK), lambda j, h, m: (0, block(j, h, m))),
            ]
            + [strip] * 4,
            scratch_shapes=[pltpu.VMEM((ROWS, BLK), BF)] * 2 + [pltpu.VMEM((1, HALF), F32)],
        ),
        out_shape=[
            jax.ShapeDtypeStruct((D, FF), F32),
            jax.ShapeDtypeStruct((D, FF), F32),
            jax.ShapeDtypeStruct((FF, D), F32),
        ]
        + [pltpu.HBM((TOK, HALF), F32)] * 4,
        compiler_params=vm(18),
        cost_estimate=pl.CostEstimate(
            flops=3 * 2 * ROWS * D * FF, bytes_accessed=20_000_000, transcendentals=0
        ),
    )(meta, *in_hbm(perm, own, peer, hid, gg, gu, gate_pre, lru_out, log_decay))


def combine_kernel(
    meta, ids_hbm, ret, d_hbm, w_hbm, dm_ref, b0, b1, b2, b3, w_ref, ids, own, sems
):
    tp, z = meta[0], meta[1]
    cut = SLOTS // 4
    copies = fetch(
        [(ids_hbm, ids)]
        + [(d_hbm.at[:, lanes(2 * j + tp)], own.at[:, j * BLK : (j + 1) * BLK]) for j in range(4)]
        + [(w_hbm.at[:, lanes(2 * j + tp)], w_ref.at[j, :, :]) for j in range(4)]
        + [(w_hbm.at[:, lanes(2 * j + 1 - tp)], w_ref.at[4 + j, :, :]) for j in range(4)],
        sems,
    )
    copies[0].wait()
    r0, r1 = slot_rows(ids)
    c0, c1 = as_column(r0).astype(jnp.int32), as_column(r1).astype(jnp.int32)
    low = high = 0.0
    for k in range(4):
        slot = lax.broadcasted_iota(jnp.int32, (TOK, cut), 1) + k * cut
        first = jnp.where((slot == c0) | (slot == c1), 1.0, 0.0).astype(BF)
        second = jnp.where((slot == c0 + CAP) | (slot == c1 + CAP), 1.0, 0.0).astype(BF)
        piece = ret[k * cut : (k + 1) * cut, :]
        low += dot(first, piece)
        high += dot(second, piece)
    for copy in copies[1:5]:
        copy.wait()
    dm_ref[:, :512] = (own[:, :512].astype(F32) + low).astype(BF)
    dm_ref[:, 512:] = (own[:, 512:].astype(F32) + high).astype(BF)
    for k, ref in enumerate((b0, b1, b2, b3)):
        ref[...] = dm_ref[:, lanes(lax.rem(z + k, 4))]
    for copy in copies[5:]:
        copy.wait()


def combine(meta, ids, ret, d_out, w_out):
    return pl.pallas_call(
        combine_kernel,
        name="combine",
        in_specs=mixed("hvhh"),
        out_specs=[pl.BlockSpec(memory_space=pltpu.VMEM)] * 6,
        out_shape=[jax.ShapeDtypeStruct((TOK, HALF), BF)]
        + [jax.ShapeDtypeStruct((TOK, BLK), BF)] * 4
        + [jax.ShapeDtypeStruct((8, HALF, BLK), BF)],
        scratch_shapes=[
            pltpu.VMEM((2, TOK), jnp.int32),
            pltpu.VMEM((TOK, HALF), BF),
            pltpu.SemaphoreType.DMA((13,)),
        ],
        compiler_params=vm(12),
        cost_estimate=cost(1e9),
    )(meta, *in_hbm(ids), ret, *in_hbm(d_out, w_out))


def tile_of(line):
    return jnp.concatenate([line[:, k * 128 : (k + 1) * 128] for k in range(8)], axis=0)


def line_of(tile):
    return jnp.concatenate([tile[k : k + 1, :] for k in range(8)], axis=1)


def early_kernel(gate_ref, lru_ref, gated_ref):
    value, _ = gelu_parts(gate_ref[...].astype(F32))
    gated_ref[...] = (value * lru_ref[...].astype(F32)).astype(BF)


def early(gate_pre, lru_out):
    return pl.pallas_call(
        early_kernel,
        name="early",
        out_shape=jax.ShapeDtypeStruct((TOK, HALF), BF),
        compiler_params=vm(4),
        cost_estimate=cost(1e8),
    )(gate_pre, lru_out)


def scan_rows(drive_ref, rate_ref, start, visit):
    carry = start
    for tile in reversed(range(TOK // 8)):
        rows = slice(tile * 8, tile * 8 + 8)
        drive, rate = drive_ref[rows, :], rate_ref[rows, :]
        here, later = [None] * 8, [None] * 8
        for r in reversed(range(8)):
            here[r] = drive[r : r + 1] + carry
            carry = rate[r : r + 1] * here[r]
            later[r] = carry
        if visit is not None:
            visit(rows, jnp.concatenate(here, axis=0), jnp.concatenate(later, axis=0))
    return carry


def drive_kernel(
    meta, own_ref, peer_ref, w_ref, value_hbm, slope_hbm, rate_hbm, after_hbm, g0, g1, g2, g3,
    dgate_ref, local_ref, head_ref, moved_ref, value, slope, rate, after, sems,
):
    copies = fetch(
        [
            (value_hbm, value),
            (rate_hbm, rate),
            (after_hbm.at[0:8, :], after),
            (slope_hbm, slope),
        ]
        + [(g, moved_ref.at[k, :, :]) for k, g in enumerate((g0, g1, g2, g3))],
        sems,
    )
    grad = 0.0
    for k in range(8):
        ref, j = (own_ref, peer_ref)[k // 4], k % 4
        grad += dot_cols(ref[:, j * BLK : (j + 1) * BLK], w_ref[k, :, :])
    copies[0].wait()
    local_ref[...] = grad * value[...]
    for copy in copies[1:4]:
        copy.wait()
    dgate_ref[...] = (grad * slope[...]).astype(BF)

    def visit(rows, here, later):
        local_ref[rows, :] = here

    head_ref[0:8, :] = tile_of(scan_rows(local_ref, rate, jnp.zeros((1, HALF), F32), visit))
    head_ref[8:16, :] = tile_of(after[0:1, :] * rate[0:1, :])
    for copy in copies[4:]:
        copy.wait()


def drive(meta, own, peer, w, value, slope, rate, after, gated):
    wide = pltpu.VMEM((TOK, HALF), F32)
    return pl.pallas_call(
        drive_kernel,
        name="drive",
        in_specs=mixed("vvvhhhhaaaa"),
        out_specs=[pl.BlockSpec(memory_space=pltpu.VMEM)] * 4,
        out_shape=[
            jax.ShapeDtypeStruct((TOK, HALF), BF),
            jax.ShapeDtypeStruct((TOK, HALF), F32),
            jax.ShapeDtypeStruct((16, 128), F32),
            jax.ShapeDtypeStruct((4, TOK, HALF), BF),
        ],
        scratch_shapes=[wide, wide, wide, pltpu.VMEM((8, HALF), F32), pltpu.SemaphoreType.DMA((8,))],
        compiler_params=vm(12),
        cost_estimate=cost(2e9),
    )(meta, own, peer, w, *in_hbm(value, slope, rate, after), *gated)


def link_kernel(meta, shares_ref, within_ref, after_ref, plane_ref):
    place = meta[3]
    within = jnp.zeros((8, 128), F32)
    total = jnp.zeros((8, 128), F32)
    after = jnp.ones((8, 128), F32)
    product = jnp.ones((8, 128), F32)
    for r in reversed(range(16)):
        tile = shares_ref[r, :, HALF:].astype(F32)
        head, block = tile[0:8] + tile[8:16], tile[16:24] + tile[24:32]
        total = head + block * total
        product = block * product
        within = jnp.where(place < r, total, within)
        after = jnp.where(place < r, product, after)
    within_ref[...] = within
    after_ref[...] = after
    plane_ref[0:8, :] = total
    plane_ref[8:16, :] = product


def link(meta, shares):
    return pl.pallas_call(
        link_kernel,
        name="link",
        in_specs=whole(1),
        out_specs=[pl.BlockSpec(memory_space=pltpu.VMEM)] * 3,
        out_shape=[
            jax.ShapeDtypeStruct((8, 128), F32),
            jax.ShapeDtypeStruct((8, 128), F32),
            jax.ShapeDtypeStruct((16, 128), F32),
        ],
        compiler_params=vm(8),
        cost_estimate=cost(1e7),
    )(meta, shares)


def finish_kernel(
    within_ref, after_ref, p1, p2, p3, local_ref, suffix_ref, rate_ref, lru_ref, before_ref,
    dd_ref, dl_ref,
):
    planes = p3[0:8, :]
    planes = p2[0:8, :] + p2[8:16, :] * planes
    planes = p1[0:8, :] + p1[8:16, :] * planes
    incoming = line_of(within_ref[...] + after_ref[...] * planes)
    value = local_ref[...] + suffix_ref[...] * incoming
    dd_ref[...] = value
    first = lax.broadcasted_iota(jnp.int32, (TOK, HALF), 0) == 0
    state = pltpu.roll(lru_ref[...].astype(F32), 1, 0)
    dl_ref[...] = value * rate_ref[...] * jnp.where(first, before_ref[...].astype(F32), state)


def finish(within, after, planes, local, suffix, rate, lru_out, before):
    return pl.pallas_call(
        finish_kernel,
        name="finish",
        out_shape=[jax.ShapeDtypeStruct((TOK, HALF), F32)] * 2,
        compiler_params=vm(8),
        cost_estimate=cost(1e9),
    )(within, after, *planes, local, suffix, rate, lru_out, before)


def outer_own_kernel(b0, b1, b2, b3, moved, out_ref):
    total = 0.0
    for k, ref in enumerate((b0, b1, b2, b3)):
        total += dot_rows(ref[...], moved[k, :, :])
    out_ref[...] = total.astype(BF)


def outer_own(blocks, moved):
    return pl.pallas_call(
        outer_own_kernel,
        name="outer_own",
        in_specs=mixed("vvvvv")[1:],
        out_specs=pl.BlockSpec(memory_space=pltpu.VMEM),
        out_shape=jax.ShapeDtypeStruct((BLK, HALF), BF),
        compiler_params=vm(8),
        cost_estimate=cost(1e9),
    )(*blocks, moved)


def outer_kernel(meta, p0, p1, p2, p3, moved, own_ref, head_ref, out_ref):
    tp, z = meta[0], meta[1]
    out_ref[lanes(tp), 0:HALF] = own_ref[...]
    value = head_ref[...]
    high = value.astype(BF).astype(F32)
    low = value - high
    tile = jnp.concatenate([high[0:8], low[0:8], high[8:16], low[8:16]], axis=0).astype(BF)
    for k in range(16):
        out_ref[k * 32 : (k + 1) * 32, HALF:] = tile
    total = dot_rows(p0[:, lanes(z)], moved[0, :, :])
    for k, ref in ((1, p1), (2, p2), (3, p3)):
        total += dot_rows(ref[...], moved[k, :, :])
    out_ref[lanes(1 - tp), 0:HALF] = total.astype(BF)


def outer(meta, peer, moved, own, head):
    return pl.pallas_call(
        outer_kernel,
        name="outer",
        in_specs=mixed("vvvvvvv"),
        out_specs=pl.BlockSpec(memory_space=pltpu.VMEM),
        out_shape=jax.ShapeDtypeStruct((2 * BLK, HALF + 128), BF),
        compiler_params=vm(8),
        cost_estimate=cost(1e9),
    )(meta, *peer, moved, own, head)


def swapped(value):
    return lax.ppermute(value, "tp", [(0, 1), (1, 0)])


def turned(value, steps):
    return lax.ppermute(value, "z", [(s, (s + steps) % 4) for s in range(4)])


def on_device(
    stream_mid, d_out, route_ids, route_weights, gate_pre, lru_out, log_decay, w_out,
    exp_gate, exp_up, exp_down,
):
    meta = jnp.stack(
        [lax.axis_index("tp"), lax.axis_index("z"), lax.axis_index(SP), lax.axis_index(("y", "x"))]
    ).astype(jnp.int32)
    perm, perm_t = jnp.asarray(_perm, BF), jnp.asarray(_perm.T, BF)
    ids = route_ids.T
    wg, wu, wd = exp_gate[0], exp_up[0], exp_down[0]
    sent = pack(meta, ids, route_weights.T, stream_mid, d_out)
    got = lax.all_to_all(sent.reshape(NSP, CHUNK, HALF), SP, 0, 0, tiled=True)
    got = got.reshape(SLOTS, HALF)
    got_peer = swapped(got)
    gated = early(gate_pre, lru_out)
    gated, got = lax.optimization_barrier((gated, got))
    turn2 = turned(gated, 2)
    pg, pu, pb = expert_own(meta, perm, got, wg, wu, wd)
    hid, gg, gu, part_peer = expert_peer(meta, perm, perm_t, got_peer, wg, wu, wd, pg, pu, pb)
    other = swapped(part_peer)
    part_own = expert_back(meta, perm_t, gg, gu, wg, wu)
    back = part_sum(part_own, other)
    back, turn2 = lax.optimization_barrier((back, turn2))
    ret = lax.all_to_all(back.reshape(NSP, CHUNK, HALF // 2), SP, 0, 0, tiled=True)
    back, moving, last = lax.optimization_barrier((back, gated, lru_out[-1:]))
    turn1, turn3 = turned(moving, 1), turned(moving, 3)
    before = lax.ppermute(last, SP, [(s, s + 1) for s in range(NSP - 1)])
    grads = weight_grads(
        meta, perm, got, got_peer, hid, gg, gu, gate_pre, lru_out, log_decay
    )
    ret, *grads = lax.optimization_barrier((ret, *grads))
    grad_gate, grad_up, grad_down, value, slope, rate, suffix = grads
    dm, *blocks, w = combine(meta, ids, ret.reshape(SLOTS, HALF // 2), d_out, w_out)
    dm_peer = swapped(dm)
    own = (blocks[0], *(turned(blocks[k], k) for k in (1, 2, 3)))
    d_gate, local, head, moved = drive(
        meta, dm, dm_peer, w, value, slope, rate, suffix, (gated, turn1, turn2, turn3)
    )
    peer = (dm_peer, *(swapped(own[k]) for k in (1, 2, 3)))
    share = outer(meta, peer, moved, outer_own(own, moved), head)
    shares = lax.all_to_all(share.reshape(16, 32, HALF + 128), ("y", "x"), 0, 0, tiled=True)
    within, after, plane = link(meta, shares)
    planes = [lax.ppermute(plane, "z", [(s, s - k) for s in range(k, 4)]) for k in (1, 2, 3)]
    d_drive, d_log_decay = finish(
        within, after, planes, local, suffix, rate, lru_out, before
    )
    grad_out_proj = jnp.sum(shares[:, :, :HALF].astype(F32), axis=0)
    return (
        grad_gate[None], grad_up[None], grad_down[None], grad_out_proj, d_gate, d_drive, d_log_decay,
    )


def solution(mesh):
    fine = Mesh(mesh.devices.reshape(4, 4, 4, 2), ("z", "y", "x", "tp"))
    tokens = P(SP, None)
    both = P(SP, "tp")
    hidden = P(SP, None, "tp")
    in_specs = (
        tokens, tokens, tokens, tokens, both, both, both, P("tp", None),
        hidden, hidden, P(SP, "tp", None),
    )
    out_specs = (hidden, hidden, P(SP, "tp", None), both, both, both, both)
    return jax.shard_map(
        on_device, mesh=fine, in_specs=in_specs, out_specs=out_specs, check_vma=False
    )
```
